128 devices in a mesh: sp: 32 (over z, y, core), tp: 4 (over x).
Axes of the slice: x: 4, y: 4, z: 4, core: 2. Of those that a mesh axis runs over, the one named last changes fastest.
Arguments:
- stream: bfloat16 [8192, 2048], P('sp'), may hold values from -6 to 6
- narrow_query_weight: bfloat16 [8192, 1024], P('sp', 'tp'), may hold values from -6 to 6
- wide_query_weight: bfloat16 [8192, 2048], P('sp', 'tp'), may hold values from -6 to 6
- value_rows_heads: bfloat16 [8192, 2, 1024], P('sp', None, 'tp'), may hold values from -6 to 6
- output_gate_logits: bfloat16 [8192, 2, 1024], P('sp', None, 'tp'), may hold values from -6 to 6
- narrow_forget_logits: bfloat16 [2, 8192, 1024], P(None, 'sp', 'tp'), may hold values from -6 to 6
- wide_forget_logits: bfloat16 [2, 8192, 2048], P(None, 'sp', 'tp'), may hold values from -6 to 6
- narrow_forget_headroom: float32 [2, 1024], P(None, 'tp'), may hold values from 0 to 0.08, as said below
- wide_forget_headroom: float32 [2, 2048], P(None, 'tp'), may hold values from 0 to 0.08, as said below
- extra_log_decay: float32 [8192, 2, 16], P('sp', None, 'tp'), may hold values from -1.4 to 0
- per_head_norm_gain: float32 [64], replicated, may hold values from 0.1 to 1.9
- mixer_output_weight: bfloat16 [2, 1024, 2048], replicated, may hold values from -0.125 to 0.125
- feedforward_norm_gain: float32 [2048], replicated, may hold values from 0.1 to 1.9
- expert_gate_matrix: bfloat16 [32, 2048, 4096], P('sp', None, 'tp'), may hold values from -0.125 to 0.125
- expert_up_matrix: bfloat16 [32, 2048, 4096], P('sp', None, 'tp'), may hold values from -0.125 to 0.125
- expert_down_matrix: bfloat16 [32, 4096, 2048], P('sp', 'tp'), may hold values from -0.09375 to 0.09375
- routes: int32 [8192, 2], P('sp'), may hold values from 0 to 31, all different within a row; in each aligned block of 64 rows (0 to 63, 64 to 127, ...) at most 8 rows name the same one
- router_scores_chosen: float32 [8192, 2], P('sp'), may hold values from -8 to 8
Outputs:
- result: bfloat16 [8192, 2048], P(('sp', 'tp'))
The draws below stay inside these ranges and needn't reach their ends.
Inputs may be any that keep to these rules, and one draw needn't show every extreme that they name: `routes`: each row names 2 different experts; in each aligned block of 64 rows no expert is named by more than 8 rows. `narrow_forget_headroom`: positive. `wide_forget_headroom`: positive.
All inputs are finite; a program needn't handle non-finite values.
Results may differ from the reference program's by a relative error of at most 0.011.
Values may be sent and summed in bfloat16 or wider, within the bound.
No kernel may reach another device: no remote copies, remote signals or barrier semaphores. Data moves between devices by JAX's collectives and lax.ppermute only.
A program may use at most 128 MiB of HBM per device.

```python
import math
from functools import partial
import jax
import jax.numpy as jnp
import numpy as np
from jax import lax

D = 2048
HG = 16
DV = 64
DKN = 64
DKW = 128
FF_EXP = 4096
TOP = 2
BLOCK = 64
TOK_DEV = 256
TOKENS = 8192
ROWS = 64
EXPERTS = 32
CAP = 8
N_TP = 4


def forget_field(key, state_rows):
    first_key, second_key = jax.random.split(jax.random.fold_in(key, 17))
    device_spans = TOKENS // TOK_DEV
    full_shape = (2, TOKENS, HG * state_rows)
    offsets = jax.random.uniform(first_key, (2, device_spans, 1), jnp.float32, -1.2, 1.2)
    jitter = jnp.clip(jax.random.normal(second_key, full_shape, jnp.float32), -4.0, 4.0)
    return (jnp.repeat(offsets, TOK_DEV, axis=1) + jitter).astype(jnp.bfloat16)


def room_field(key, state_rows):
    subkeys = jax.random.split(jax.random.fold_in(key, 29), 3)
    quick_share = 0.5
    is_quick = jax.random.bernoulli(subkeys[0], quick_share, (2, HG, 1))
    quick_room = jnp.exp(jax.random.uniform(subkeys[1], (2, HG, state_rows), jnp.float32, jnp.log(0.04), jnp.log(0.08)))
    lasting_room = jax.random.uniform(subkeys[2], (2, HG, state_rows), jnp.float32, 0.2, 0.7) * (2.0 / TOKENS)
    return jnp.where(is_quick, quick_room, lasting_room).reshape(2, HG * state_rows).astype(jnp.float32)


def draw_narrow_forget_logits(key, part):
    return forget_field(key, DKN)


def draw_wide_forget_logits(key, part):
    return forget_field(jax.random.fold_in(key, 5), DKW)


def draw_narrow_forget_headroom(key, part):
    return room_field(key, DKN)


def draw_wide_forget_headroom(key, part):
    return room_field(jax.random.fold_in(key, 7), DKW)


def draw_extra_log_decay(key, part):
    first_key, second_key = jax.random.split(jax.random.fold_in(key, 43))
    positions = jax.random.randint(first_key, (2, 2, HG), 0, TOKENS)
    losses = jnp.log(jax.random.uniform(second_key, (2, 2, HG), jnp.float32, 0.5, 0.8))
    matches = jnp.arange(TOKENS)[:, None, None, None] == positions[None]
    return jnp.sum(jnp.where(matches, losses[None], 0.0), axis=1).astype(jnp.float32)


def levels(rng, extent, shards, smallest, top_value):
    factor_of = 1.0
    for axis_at, parts in shards:
        steps = jax.random.uniform(jax.random.fold_in(jax.random.fold_in(rng, 6), axis_at), (parts,), jnp.float32, smallest / len(shards), top_value / len(shards))
        factor_of = factor_of * jnp.repeat(jnp.exp(steps), extent[axis_at] // parts).reshape((-1,) + (1,) * (len(extent) - 1 - axis_at))
    return factor_of


def routed_block(rng, own, number, rows, number_of, top, reach, skew):
    order = jax.random.permutation(rng, number_of)
    heavy_load, common = shares(number_of, rows * top, reach, skew, True), shares(number_of, rows * top, reach, skew, False)
    places = jnp.arange(number_of)

    def named(lengths, turn):
        used = int((lengths > 0).sum())
        fixed = max(1, used // 4)
        shifted = fixed + (places - fixed + turn * (used - fixed)) % max(1, number_of - fixed)
        return jnp.zeros((number_of,), jnp.int32).at[order[jnp.where(places < fixed, places, shifted)]].set(jnp.asarray(lengths, jnp.int32))

    lengths = jnp.where(number % 4 == 0, named(heavy_load, number // 4), named(common, number - number // 4 - 1))
    mixed = jax.random.permutation(jax.random.fold_in(own, 3), number_of)
    donor, receiver = mixed[0:number_of // 2 * 2:2], mixed[1:number_of // 2 * 2:2]
    room = jnp.minimum(lengths[donor] - 1, reach - lengths[receiver]) // 2
    room = jnp.where((donor == order[0]) | (receiver == order[0]) | (lengths[receiver] == 0), 0, jnp.maximum(room, 0))
    shifted = jax.random.randint(jax.random.fold_in(own, 4), (number_of // 2,), 0, 1 << 20) % (room + 1)
    lengths = lengths.at[donor].add(-shifted).at[receiver].add(shifted)
    labels = jnp.searchsorted(jnp.cumsum(lengths), jnp.arange(rows * top), side="right").astype(jnp.int32)
    grid = labels.reshape(top, rows).T
    grid = grid[jax.random.permutation(jax.random.fold_in(own, 1), rows)]
    turn = jax.random.randint(jax.random.fold_in(own, 2), (rows, 1), 0, top)
    return jnp.take_along_axis(grid, (jnp.arange(top)[None, :] + turn) % top, axis=1)


def shares(number_of, total, reach, lean, full):
    loads = [(1 << 20) // math.isqrt(grade ** lean) + 1 for grade in range(1, number_of + 1)]
    largest = reach if full else min(reach, max(-(-total // number_of), total * loads[0] // sum(loads)))
    least = 1 if total - largest >= number_of - 1 else 0
    given, rest = [largest] + [least] * (number_of - 1), total - largest - least * (number_of - 1)
    while rest > 0:
        candidates = [i for i in range(1, number_of) if given[i] < largest] or [i for i in range(1, number_of) if given[i] < reach]
        mass, left = sum([loads[i] for i in candidates]), rest
        for i in candidates:
            extra = min(reach - given[i], max(1, left * loads[i] // mass), rest)
            given[i] = given[i] + extra
            rest = rest - extra
    return np.array(given)


def normal_values(rng, extent, spread, limit, cuts=(), held_as=jnp.bfloat16):
    loudness = levels(rng, extent, cuts, -0.22, 0.18) if cuts else 1.0
    entries = jax.random.normal(rng, extent, jnp.float32) * spread * loudness
    return jnp.minimum(jnp.maximum(entries, -limit), limit).astype(held_as)


def setup_inputs(seed: int = 0) -> dict:
    seeds = jax.random.split(jax.random.key(seed), 19)
    stream = normal_values(seeds[0], (TOKENS, D), 1.0, 6.0, ((0, 32),))
    narrow_query_weight = normal_values(seeds[1], (TOKENS, HG * DKN), 1.0, 6.0, ((0, 32), (1, 4)))
    wide_query_weight = normal_values(seeds[2], (TOKENS, HG * DKW), 1.0, 6.0, ((0, 32), (1, 4)))
    value_rows_heads = normal_values(seeds[3], (TOKENS, 2, HG * DV), 1.0, 6.0, ((0, 32), (2, 4)))
    output_gate_logits = normal_values(seeds[4], (TOKENS, 2, HG * DV), 1.0, 6.0, ((0, 32), (2, 4)))
    narrow_forget_logits = draw_narrow_forget_logits(jax.random.fold_in(seeds[18], 71), 0)
    wide_forget_logits = draw_wide_forget_logits(jax.random.fold_in(seeds[18], 71), 0)
    narrow_forget_headroom = draw_narrow_forget_headroom(jax.random.fold_in(seeds[18], 71), 0)
    wide_forget_headroom = draw_wide_forget_headroom(jax.random.fold_in(seeds[18], 71), 0)
    extra_log_decay = draw_extra_log_decay(jax.random.fold_in(seeds[18], 71), 0)
    per_head_norm_gain = jnp.clip(1.0 + 0.18 * jax.random.normal(seeds[10], (DV,), jnp.float32), 0.1, 1.9)
    mixer_output_weight = normal_values(seeds[11], (2, HG * DV, D), (2 * HG * DV) ** -0.5, 0.125)
    feedforward_norm_gain = jnp.clip(1.0 + 0.18 * jax.random.normal(seeds[12], (D,), jnp.float32), 0.1, 1.9)
    expert_gate_matrix = normal_values(seeds[13], (EXPERTS, D, FF_EXP), D ** -0.5, 0.125, ((0, 32), (2, 4)))
    expert_up_matrix = normal_values(seeds[14], (EXPERTS, D, FF_EXP), D ** -0.5, 0.125, ((0, 32), (2, 4)))
    expert_down_matrix = normal_values(seeds[15], (EXPERTS, FF_EXP, D), FF_EXP ** -0.5, 0.09375, ((0, 32), (1, 4)))
    routes_keys = jax.random.split(jax.random.fold_in(seeds[16], 1), TOKENS // ROWS)
    routes_turns = jax.random.permutation(jax.random.fold_in(seeds[16], 3), TOKENS // ROWS)
    routes = jax.vmap(lambda own, number: routed_block(jax.random.fold_in(seeds[16], 2), own, number, ROWS, EXPERTS, TOP, CAP, 2))(routes_keys, routes_turns).reshape((TOKENS, TOP))
    router_scores_chosen = normal_values(seeds[17], (TOKENS, TOP), 2.0, 8.0, ((0, 32),), jnp.float32)
    return {"stream": stream, "narrow_query_weight": narrow_query_weight, "wide_query_weight": wide_query_weight, "value_rows_heads": value_rows_heads, "output_gate_logits": output_gate_logits, "narrow_forget_logits": narrow_forget_logits, "wide_forget_logits": wide_forget_logits, "narrow_forget_headroom": narrow_forget_headroom, "wide_forget_headroom": wide_forget_headroom, "extra_log_decay": extra_log_decay, "per_head_norm_gain": per_head_norm_gain, "mixer_output_weight": mixer_output_weight, "feedforward_norm_gain": feedforward_norm_gain, "expert_gate_matrix": expert_gate_matrix, "expert_up_matrix": expert_up_matrix, "expert_down_matrix": expert_down_matrix, "routes": routes, "router_scores_chosen": router_scores_chosen}


EPS = 1e-06
TOP_PRECISION = lax.Precision.HIGHEST

def block_sweep(query_rows, block_openings, values, decay_logarithm):
    token_rows, total_head_count, state_rows = query_rows.shape
    value_size = values.shape[2]
    blocks = token_rows // BLOCK

    def to_blocks(source):
        return source.reshape(blocks, BLOCK, total_head_count, source.shape[2]).transpose(0, 2, 1, 3)
    inside = jnp.cumsum(to_blocks(decay_logarithm), axis=2)
    triangle = jnp.tril(jnp.ones((BLOCK, BLOCK), jnp.float32))

    def advance(present_state, inputs):
        block_of_queries, block_opening_state, block_of_values, inside_block = inputs
        ending = inside_block[:, -1:, :]
        query_within_block = block_of_queries * jnp.exp(inside_block)
        k_inside = block_opening_state * jnp.exp(-inside_block)
        key_block_ending = block_opening_state * jnp.exp(ending - inside_block)
        scores = jnp.einsum('htk,hsk->hts', query_within_block, k_inside, precision=TOP_PRECISION) * triangle
        final_output = jnp.einsum('hts,hsv->htv', scores, block_of_values, precision=TOP_PRECISION)
        final_output = final_output + jnp.einsum('ifm,imo->ifo', query_within_block, present_state, precision=TOP_PRECISION)
        expanded_state = jnp.einsum('lbi,lbp->lip', key_block_ending, block_of_values, precision=TOP_PRECISION)
        present_state = present_state * jnp.exp(ending[:, 0, :])[:, :, None] + expanded_state
        return (present_state, final_output)
    zero_state = jnp.zeros((total_head_count, state_rows, value_size), jnp.float32)
    closing_state, outputs = lax.scan(advance, zero_state, (to_blocks(query_rows), to_blocks(block_openings), to_blocks(values), inside))
    return outputs.transpose(0, 2, 1, 3).reshape(token_rows, total_head_count, value_size)

def slot_table(block_routes, experts, capacity):
    flattened = block_routes.reshape(-1)
    matches = (flattened[:, None] == jnp.arange(experts, dtype=jnp.int32)[None, :]).astype(jnp.int32)
    earlier = jnp.cumsum(matches, axis=0) - matches
    token_position = lax.optimization_barrier(jnp.sum(earlier * matches, axis=1)).astype(jnp.int32)
    return (flattened * capacity + token_position).reshape(block_routes.shape)

def reference(stream, narrow_query_weight, wide_query_weight, value_rows_heads, output_gate_logits, narrow_forget_logits, wide_forget_logits, narrow_forget_headroom, wide_forget_headroom, extra_log_decay, per_head_norm_gain, mixer_output_weight, feedforward_norm_gain, expert_gate_matrix, expert_up_matrix, expert_down_matrix, routes, router_scores_chosen):
    groups = ((narrow_query_weight, narrow_forget_logits, narrow_forget_headroom), (wide_query_weight, wide_forget_logits, wide_forget_headroom))
    mixed_groups = []
    for head_group_index in range(2):
        query_rows, forget_gate, forget_headroom = groups[head_group_index]
        query_heads = jax.nn.silu(query_rows.astype(jnp.float32)).reshape(TOKENS, HG, -1)
        value_heads = value_rows_heads[:, head_group_index].astype(jnp.float32).reshape(TOKENS, HG, DV)
        pre_forget = forget_gate.astype(jnp.float32).reshape(2, TOKENS, HG, -1)
        block_openings = jax.nn.sigmoid(-pre_forget) * forget_headroom.reshape(2, 1, HG, -1)
        decay_logarithm = jnp.log1p(-block_openings) + extra_log_decay[None, :, head_group_index, :, None]
        ahead = block_sweep(query_heads, block_openings[0], value_heads, decay_logarithm[0])
        behind = jnp.flip(block_sweep(jnp.flip(query_heads, 0), jnp.flip(block_openings[1], 0), jnp.flip(value_heads, 0), jnp.flip(decay_logarithm[1], 0)), 0)
        summed = ahead + behind
        scale = lax.rsqrt(lax.optimization_barrier(jnp.mean(summed * summed, axis=-1, keepdims=True)) + EPS)
        gates = jax.nn.silu(output_gate_logits[:, head_group_index].astype(jnp.float32)).reshape(TOKENS, HG, DV)
        mixed_groups.append((summed * scale * per_head_norm_gain * gates).reshape(TOKENS, HG * DV))
    mixed = jnp.stack(mixed_groups, axis=1).astype(jnp.bfloat16).reshape(TOKENS, 2 * HG * DV)
    projected = jnp.dot(mixed, mixer_output_weight.reshape(2 * HG * DV, D), preferred_element_type=jnp.float32)
    residual = stream.astype(jnp.float32) + projected
    norm_rows = (residual * lax.rsqrt(lax.optimization_barrier(jnp.mean(residual * residual, axis=-1, keepdims=True)) + EPS) * feedforward_norm_gain).astype(jnp.bfloat16)
    blocks = TOKENS // ROWS
    slot_count = EXPERTS * CAP
    slot_ids = jax.vmap(partial(slot_table, experts=EXPERTS, capacity=CAP))(routes.reshape(blocks, ROWS, TOP))
    global_slots = (slot_ids + (jnp.arange(blocks, dtype=jnp.int32) * slot_count)[:, None, None]).reshape(-1)
    row_ids = jnp.repeat(jnp.arange(TOKENS, dtype=jnp.int32), TOP)
    row_table = jnp.full((blocks * slot_count,), TOKENS, jnp.int32).at[global_slots].set(row_ids)
    row_table = row_table.reshape(blocks, EXPERTS, CAP).transpose(1, 0, 2).reshape(EXPERTS, blocks * CAP)
    padded_rows = jnp.concatenate([norm_rows, jnp.zeros((1, D), jnp.bfloat16)], axis=0)
    quarter_width = FF_EXP // N_TP

    def one_expert(inputs):
        row_index, gate_weights, up_weights, down_weights = inputs
        gathered = padded_rows[row_index]
        gate_part = jnp.dot(gathered, gate_weights, preferred_element_type=jnp.float32)
        up_part = jnp.dot(gathered, up_weights, preferred_element_type=jnp.float32)
        hidden = (jax.nn.silu(gate_part) * up_part).astype(jnp.bfloat16)
        combined = jnp.zeros((gathered.shape[0], D), jnp.float32)
        for quarter in range(N_TP):
            lower_edge = quarter * quarter_width
            upper_edge = lower_edge + quarter_width
            partial_out = jnp.dot(hidden[:, lower_edge:upper_edge], down_weights[lower_edge:upper_edge], preferred_element_type=jnp.float32).astype(jnp.bfloat16)
            combined = combined + lax.optimization_barrier(partial_out).astype(jnp.float32)
        return combined.astype(jnp.bfloat16)
    expert_out = lax.map(one_expert, (row_table, expert_gate_matrix, expert_up_matrix, expert_down_matrix))
    expert_out = expert_out.reshape(EXPERTS, blocks, CAP, D).transpose(1, 0, 2, 3).reshape(blocks * slot_count, D)
    picked = expert_out[global_slots].reshape(TOKENS, TOP, D)
    weights = jax.nn.sigmoid(router_scores_chosen - router_scores_chosen[:, ::-1])
    mixed_out = lax.optimization_barrier(jnp.sum(weights[:, :, None] * picked.astype(jnp.float32), axis=1))
    return (residual + mixed_out).astype(jnp.bfloat16)
```

```python
from functools import partial

import jax
import jax.numpy as jnp
from jax import lax
from jax.experimental import pallas as pl
from jax.experimental.pallas import tpu as pltpu
from jax.sharding import Mesh
from jax.sharding import PartitionSpec as P

SP = ("sp_0", "sp_1", "sp_2")
SP_TP = ("sp_0", "sp_1", "sp_2", "tp")

EPS = 1e-06
F32 = jnp.float32
BF16 = jnp.bfloat16

TOK = 256
BLK = 64
NB = TOK // BLK
LANES = 128
TILES = 6
STATE_ROWS = 2 * TILES * 64
PAY_ROWS = STATE_ROWS + 32


def dot(a, b):
    return lax.dot_general(a, b, (((1,), (0,)), ((), ())), preferred_element_type=F32)


def dot_t(a, b):
    return lax.dot_general(a, b, (((1,), (1,)), ((), ())), preferred_element_type=F32)


def silu(x):
    return x / (1.0 + jnp.exp(-x))


def local_kernel(
    nq_ref, wq_ref, nf_ref, wf_ref, nh_ref, wh_ref, ex_ref, v0_ref, v1_ref, pay_ref, out_ref, qr_ref
):
    ri = lax.broadcasted_iota(jnp.int32, (TOK, TOK), 0)
    ci = lax.broadcasted_iota(jnp.int32, (TOK, TOK), 1)
    same = (ri // BLK) == (ci // BLK)
    tri = (same & (ci <= ri), same & (ci >= ri))
    ones = tuple(jnp.where(t, 1.0, 0.0).astype(BF16) for t in tri)
    lane = lax.broadcasted_iota(jnp.int32, (1, LANES), 1)
    low = lane < 64
    low2 = (lax.broadcasted_iota(jnp.int32, (1, 2 * LANES), 1) % LANES) < 64
    decays = [None] * (2 * TILES)

    def prepare(tile, q_raw, f_raw, rooms, extra):
        q = silu(q_raw.astype(F32)).reshape(NB, BLK, LANES)
        qi, ki, ke, qr, ends = [], [], [], [], []
        for d in range(2):
            opening = rooms[d] / (1.0 + jnp.exp(f_raw[d].astype(F32)))
            ld = jnp.log(1.0 - opening) + extra
            hi = ld.astype(BF16)
            lo = (ld - hi.astype(F32)).astype(BF16)
            both = dot(ones[d], jnp.concatenate([hi, lo], axis=1))
            inside = (both[:, :LANES] + both[:, LANES:]).reshape(NB, BLK, LANES)
            opening = opening.reshape(NB, BLK, LANES)
            edge = BLK - 1 if d == 0 else 0
            end = [inside[b, edge : edge + 1, :] for b in range(NB)]
            start = [None] * NB
            run = jnp.zeros((1, LANES), F32)
            for b in range(NB) if d == 0 else reversed(range(NB)):
                start[b] = run
                run = run + end[b]
            decays[d * TILES + tile] = jnp.exp(run)
            start4 = jnp.stack(start, axis=0)
            end4 = jnp.stack(end, axis=0)
            qi.append((q * jnp.exp(inside)).reshape(TOK, LANES))
            qr.append((q * jnp.exp(inside + start4)).reshape(TOK, LANES).astype(BF16))
            ki.append((opening * jnp.exp(-inside)).reshape(TOK, LANES))
            ke.append((opening * jnp.exp(end4 - inside)).reshape(TOK, LANES).astype(BF16))
            ends.append([jnp.exp(e) for e in end])
        qr_ref[tile] = jnp.concatenate(qr, axis=1)
        return qi, ki, jnp.concatenate(ke, axis=1), ends

    def block_states(tile, kv, ends):
        states = [[None, None] for _ in range(NB)]
        for d in range(2):
            run = jnp.zeros((64, LANES), F32)
            for b in range(NB) if d == 0 else reversed(range(NB)):
                states[b][d] = run
                run = run * ends[d][b] + kv[b * 64 : b * 64 + 64, d * LANES : (d + 1) * LANES]
            row = (d * TILES + tile) * 64
            pay_ref[row : row + 64, :] = run.astype(BF16)
        return [jnp.concatenate(s, axis=1) for s in states]

    def transposed(v):
        return jnp.transpose(v.astype(F32))

    def spread(vt):
        return jnp.where(same, jnp.concatenate([vt] * NB, axis=0), 0.0).astype(BF16)

    def scores(qi, ki):
        total = jnp.where(tri[0], dot_t(qi[0].astype(BF16), ki[0].astype(BF16)), 0.0)
        total = total + jnp.where(tri[1], dot_t(qi[1].astype(BF16), ki[1].astype(BF16)), 0.0)
        return total.astype(BF16)

    for p in range(2):
        cols = slice(p * LANES, (p + 1) * LANES)
        v = v0_ref[:, cols]
        extra = jnp.where(low, ex_ref[:, 2 * p : 2 * p + 1], ex_ref[:, 2 * p + 1 : 2 * p + 2])
        qi, ki, ke, ends = prepare(
            p, nq_ref[:, cols], (nf_ref[0, :, cols], nf_ref[1, :, cols]),
            (nh_ref[0:1, cols], nh_ref[1:2, cols]), extra,
        )
        vt = transposed(v)
        kv = jnp.where(low2, dot(spread(vt[:64]), ke), dot(spread(vt[64:]), ke))
        states = block_states(p, kv, ends)
        q_cat = jnp.concatenate([x.astype(BF16) for x in qi], axis=1)
        parts = []
        for b in range(NB):
            s = jnp.concatenate(
                [jnp.where(low2, states[b], 0.0), jnp.where(low2, 0.0, states[b])], axis=0
            )
            parts.append(dot_t(q_cat[b * BLK : (b + 1) * BLK], s.astype(BF16)))
        first = dot(scores(qi, [jnp.where(low, k, 0.0) for k in ki]), v)
        second = dot(scores(qi, [jnp.where(low, 0.0, k) for k in ki]), v)
        out_ref[p] = jnp.where(low, first, second) + jnp.concatenate(parts, axis=0)

    for p in range(2):
        v = v1_ref[:, p * LANES : (p + 1) * LANES]
        vt = transposed(v)
        inner, q_cats, head_states = [], [], []
        for i in range(2):
            h = 2 * p + i
            cols = slice(h * LANES, (h + 1) * LANES)
            qi, ki, ke, ends = prepare(
                2 + h, wq_ref[:, cols], (wf_ref[0, :, cols], wf_ref[1, :, cols]),
                (wh_ref[0:1, cols], wh_ref[1:2, cols]), ex_ref[:, 4 + h : 5 + h],
            )
            kv = dot(spread(vt[i * 64 : i * 64 + 64]), ke)
            head_states.append(block_states(2 + h, kv, ends))
            q_cats.append(jnp.concatenate([x.astype(BF16) for x in qi], axis=1))
            inner.append(dot(scores(qi, ki), v))
        parts = []
        for b in range(NB):
            s = jnp.concatenate([head_states[0][b], head_states[1][b]], axis=0).astype(BF16)
            rows = slice(b * BLK, (b + 1) * BLK)
            parts.append(
                jnp.where(low, dot_t(q_cats[0][rows], s), dot_t(q_cats[1][rows], s))
            )
        out_ref[2 + p] = jnp.where(low, inner[0], inner[1]) + jnp.concatenate(parts, axis=0)

    pad = jnp.zeros((16 - 2 * TILES, LANES), F32)
    dec = jnp.concatenate(decays + [pad], axis=0)
    high = dec.astype(BF16)
    pay_ref[STATE_ROWS : STATE_ROWS + 16, :] = high
    pay_ref[STATE_ROWS + 16 : STATE_ROWS + 32, :] = (dec - high.astype(F32)).astype(BF16)


def level_kernel(count, has_carry, last, here_ref, pieces_ref, *refs):
    here = here_ref[0]
    refs = list(refs)
    carry_s, carry_d = (refs.pop(0), refs.pop(0)) if has_carry else (None, None)
    if last:
        (in_ref,) = refs
    else:
        s_ref, d_ref, pay_ref = refs
    dec = [
        pieces_ref[k, STATE_ROWS : STATE_ROWS + 16, :].astype(F32)
        + pieces_ref[k, STATE_ROWS + 16 : STATE_ROWS + 32, :].astype(F32)
        for k in range(count)
    ]
    totals, inner = [], []
    for t in range(2 * TILES):
        rows = slice(t * 64, t * 64 + 64)
        order = list(range(count)) if t < TILES else list(reversed(range(count)))
        run = jnp.zeros((64, LANES), F32)
        run_d = jnp.ones((1, LANES), F32)
        mine, mine_d = run, run_d
        for k in order:
            mine = jnp.where(here == k, run, mine)
            mine_d = jnp.where(here == k, run_d, mine_d)
            if last and k == order[-1]:
                break
            d = dec[k][t : t + 1]
            run = run * d + pieces_ref[k, rows, :].astype(F32)
            run_d = run_d * d
        if has_carry:
            cd = carry_d[t : t + 1, :]
            mine = mine * cd + carry_s[rows, :]
            mine_d = mine_d * cd
        if last:
            in_ref[rows, :] = mine.astype(BF16)
        else:
            s_ref[rows, :] = mine
            pay_ref[rows, :] = run.astype(BF16)
            totals.append(run_d)
            inner.append(mine_d)
    if not last:
        pad = jnp.zeros((16 - 2 * TILES, LANES), F32)
        d_ref[...] = jnp.concatenate(inner + [pad], axis=0)
        total = jnp.concatenate(totals + [pad], axis=0)
        high = total.astype(BF16)
        pay_ref[STATE_ROWS : STATE_ROWS + 16, :] = high
        pay_ref[STATE_ROWS + 16 : STATE_ROWS + 32, :] = (total - high.astype(F32)).astype(BF16)


VMEM = pl.BlockSpec(memory_space=pltpu.VMEM)
SMEM = pl.BlockSpec(memory_space=pltpu.SMEM)


def level(axis, payload, carry, last):
    count = lax.axis_size(axis)
    pieces = lax.all_gather(payload, axis)
    here = lax.axis_index(axis).astype(jnp.int32).reshape(1)
    if last:
        shapes = jax.ShapeDtypeStruct((STATE_ROWS, LANES), BF16)
    else:
        shapes = (
            jax.ShapeDtypeStruct((STATE_ROWS, LANES), F32),
            jax.ShapeDtypeStruct((16, LANES), F32),
            jax.ShapeDtypeStruct((PAY_ROWS, LANES), BF16),
        )
    return pl.pallas_call(
        partial(level_kernel, count, carry is not None, last),
        out_shape=shapes,
        in_specs=[SMEM] + [VMEM] * (1 + (0 if carry is None else 2)),
        out_specs=VMEM if last else (VMEM,) * 3,
        name="level_" + axis,
    )(here, pieces, *(carry or ()))


def mix_kernel(out_ref, qr_ref, in_ref, g0_ref, g1_ref, gain_ref, mixed_ref):
    low = lax.broadcasted_iota(jnp.int32, (1, LANES), 1) < 64
    low2 = (lax.broadcasted_iota(jnp.int32, (1, 2 * LANES), 1) % LANES) < 64

    def entering(tile):
        a = in_ref[tile * 64 : tile * 64 + 64, :]
        b = in_ref[(TILES + tile) * 64 : (TILES + tile) * 64 + 64, :]
        return jnp.concatenate([a, b], axis=1)

    zero = jnp.zeros((64, 2 * LANES), BF16)
    for u in range(4):
        if u < 2:
            s = entering(u).astype(F32)
            s = jnp.concatenate([jnp.where(low2, s, 0.0), jnp.where(low2, 0.0, s)], axis=0)
            o = dot_t(qr_ref[u], s.astype(BF16))
        else:
            t = 2 + 2 * (u - 2)
            o = dot_t(qr_ref[t], jnp.concatenate([entering(t), zero], axis=0))
            o = o + dot_t(qr_ref[t + 1], jnp.concatenate([zero, entering(t + 1)], axis=0))
        o = o + out_ref[u]
        square = o * o
        first = jnp.sum(jnp.where(low, square, 0.0), axis=-1, keepdims=True)
        second = jnp.sum(jnp.where(low, 0.0, square), axis=-1, keepdims=True)
        scale = lax.rsqrt(jnp.where(low, first, second) * (1.0 / 64) + EPS)
        g_ref = g0_ref if u < 2 else g1_ref
        c = (u % 2) * LANES
        gate = silu(g_ref[:, c : c + LANES].astype(F32))
        mixed = o * scale * gain_ref[...] * gate
        mixed_ref[:, u * LANES : (u + 1) * LANES] = mixed.astype(BF16)


def route_kernel(
    experts, capacity, copies, own_ref, x_ref, w_ref, stream_ref, gain_ref, routes_ref, routes_t_ref,
    score_ref, res_ref, buf_ref, pick_ref, acc_ref,
):
    step = pl.program_id(0)
    part = dot(x_ref[0], w_ref[0])

    @pl.when(step == 0)
    def _():
        acc_ref[...] = stream_ref[...].astype(F32) + part

    @pl.when(step > 0)
    def _():
        acc_ref[...] += part

    @pl.when(step == pl.num_programs(0) - 1)
    def _():
        residual = acc_ref[...]
        res_ref[...] = residual
        mean = jnp.mean(residual * residual, axis=-1, keepdims=True)
        norm = (residual * lax.rsqrt(mean + EPS) * gain_ref[...]).astype(BF16)
        rows = residual.shape[0]
        col = [routes_ref[:, k : k + 1] for k in range(2)]
        row = [routes_t_ref[0, k : k + 1, :] for k in range(2)]
        ri = lax.broadcasted_iota(jnp.int32, (rows, rows), 0)
        ci = lax.broadcasted_iota(jnp.int32, (rows, rows), 1)
        earlier = ci < ri

        def count(hit):
            return jnp.sum(jnp.where(hit, 1.0, 0.0), axis=-1, keepdims=True).astype(jnp.int32)

        rank0 = count((col[0] == row[0]) & earlier)
        rank1 = count((col[1] == row[1]) & earlier) + count(col[1] == row[0])
        slot0 = col[0] * capacity + rank0
        slot1 = col[1] * capacity + rank1
        width = experts * copies * capacity
        j = lax.broadcasted_iota(jnp.int32, (rows, width), 1)
        code = (j // (copies * capacity)) * capacity + j % capacity
        hit0 = code == slot0
        hit1 = code == slot1
        s0, s1 = score_ref[:, 0:1], score_ref[:, 1:2]
        weight0 = 1.0 / (1.0 + jnp.exp(s1 - s0))
        weight1 = 1.0 / (1.0 + jnp.exp(s0 - s1))
        pick = jnp.where(hit0, weight0, 0.0) + jnp.where(hit1, weight1, 0.0)
        high = pick.astype(BF16)
        pick_ref[:rows, :] = high
        pick_ref[rows:, :] = (pick - high.astype(F32)).astype(BF16)
        chosen = jnp.where(hit0 | hit1, 1.0, 0.0)
        chosen = jnp.transpose(chosen).astype(BF16)
        buf_ref[...] = dot(chosen, norm).astype(BF16)


def final_kernel(pick_ref, back_ref, res_ref, o_ref):
    rows = res_ref.shape[0]
    both = dot(pick_ref[...], back_ref[...])
    o_ref[...] = (res_ref[...] + both[:rows] + both[rows:]).astype(BF16)


def local(
    stream,
    narrow_query_weight,
    wide_query_weight,
    value_rows_heads,
    output_gate_logits,
    narrow_forget_logits,
    wide_forget_logits,
    narrow_forget_headroom,
    wide_forget_headroom,
    extra_log_decay,
    per_head_norm_gain,
    mixer_output_weight,
    feedforward_norm_gain,
    expert_gate_matrix,
    expert_up_matrix,
    expert_down_matrix,
    routes,
    router_scores_chosen,
):
    extra = extra_log_decay.reshape(TOK, 8)
    payload, inner, q_run = pl.pallas_call(
        local_kernel,
        out_shape=(
            jax.ShapeDtypeStruct((PAY_ROWS, LANES), BF16),
            jax.ShapeDtypeStruct((4, TOK, LANES), F32),
            jax.ShapeDtypeStruct((TILES, TOK, 2 * LANES), BF16),
        ),
        in_specs=[VMEM] * 9,
        out_specs=(VMEM,) * 3,
        name="local_mixer",
    )(
        narrow_query_weight, wide_query_weight, narrow_forget_logits, wide_forget_logits,
        narrow_forget_headroom, wide_forget_headroom, extra,
        value_rows_heads[:, 0], value_rows_heads[:, 1],
    )
    s, d, payload = level("sp_2", payload, None, False)
    s, d, payload = level("sp_1", payload, (s, d), False)
    entering = level("sp_0", payload, (s, d), True)
    gain2 = jnp.concatenate([per_head_norm_gain, per_head_norm_gain]).reshape(1, LANES)
    mixed = pl.pallas_call(
        mix_kernel,
        out_shape=jax.ShapeDtypeStruct((TOK, 4 * LANES), BF16),
        in_specs=[VMEM] * 6,
        out_specs=VMEM,
        name="mix",
    )(inner, q_run, entering, output_gate_logits[:, 0], output_gate_logits[:, 1], gain2)

    tp = lax.axis_size("tp")
    rows = TOK // tp
    width = stream.shape[1]
    experts = lax.axis_size(SP)
    capacity = max(2, 2 * routes.shape[1] * rows // experts)
    slots = experts * tp * capacity
    own = lax.axis_index("tp").astype(jnp.int32).reshape(1)
    arrived = lax.all_to_all(mixed.reshape(tp, rows, 4 * LANES), "tp", 0, 0, tiled=True)
    routes_t = routes.reshape(tp, rows, 2).transpose(0, 2, 1)
    residual, buffers, pick = pl.pallas_call(
        partial(route_kernel, experts, capacity, tp),
        grid_spec=pltpu.PrefetchScalarGridSpec(
            num_scalar_prefetch=1,
            grid=(2 * tp,),
            in_specs=[
                pl.BlockSpec((1, rows, 2 * LANES), lambda i, o: (i // 2, 0, i % 2)),
                pl.BlockSpec((1, 2 * LANES, width), lambda i, o: (i % 2, i // 2, 0)),
                pl.BlockSpec((rows, width), lambda i, o: (o[0], 0)),
                pl.BlockSpec((1, width), lambda i, o: (0, 0)),
                pl.BlockSpec((rows, 2), lambda i, o: (o[0], 0)),
                pl.BlockSpec((1, 2, rows), lambda i, o: (o[0], 0, 0)),
                pl.BlockSpec((rows, 2), lambda i, o: (o[0], 0)),
            ],
            out_specs=[
                pl.BlockSpec((rows, width), lambda i, o: (0, 0)),
                pl.BlockSpec((slots, width), lambda i, o: (0, 0)),
                pl.BlockSpec((2 * rows, slots), lambda i, o: (0, 0)),
            ],
            scratch_shapes=[pltpu.VMEM((rows, width), F32)],
        ),
        out_shape=(
            jax.ShapeDtypeStruct((rows, width), F32),
            jax.ShapeDtypeStruct((slots, width), BF16),
            jax.ShapeDtypeStruct((2 * rows, slots), BF16),
        ),
        name="project_and_route",
    )(
        own, arrived, mixer_output_weight, stream, feedforward_norm_gain.reshape(1, width), routes,
        routes_t, router_scores_chosen,
    )
    tokens = lax.all_to_all(buffers, SP_TP, 0, 0, tiled=True)
    gate = jnp.dot(tokens, expert_gate_matrix[0], preferred_element_type=F32)
    up = jnp.dot(tokens, expert_up_matrix[0], preferred_element_type=F32)
    hidden = (jax.nn.silu(gate) * up).astype(BF16)
    part = jnp.dot(hidden, expert_down_matrix[0], preferred_element_type=F32).astype(BF16)
    back = lax.all_to_all(part, SP_TP, 0, 0, tiled=True)
    col = width // 4
    return pl.pallas_call(
        final_kernel,
        grid=(4,),
        in_specs=[
            pl.BlockSpec((2 * rows, slots), lambda i: (0, 0)),
            pl.BlockSpec((slots, col), lambda i: (0, i)),
            pl.BlockSpec((rows, col), lambda i: (0, i)),
        ],
        out_specs=pl.BlockSpec((rows, col), lambda i: (0, i)),
        out_shape=jax.ShapeDtypeStruct((rows, width), BF16),
        name="combine",
    )(pick, back, residual)


def solution(mesh):
    torus = Mesh(mesh.devices.reshape(4, 4, 2, mesh.shape["tp"]), ("sp_0", "sp_1", "sp_2", "tp"))
    return jax.shard_map(
        local,
        mesh=torus,
        in_specs=(
            P(SP, None),
            P(SP, "tp"),
            P(SP, "tp"),
            P(SP, None, "tp"),
            P(SP, None, "tp"),
            P(None, SP, "tp"),
            P(None, SP, "tp"),
            P(None, "tp"),
            P(None, "tp"),
            P(SP, None, "tp"),
            P(),
            P(),
            P(),
            P(SP, None, "tp"),
            P(SP, None, "tp"),
            P(SP, "tp", None),
            P(SP, None),
            P(SP, None),
        ),
        out_specs=P(SP_TP, None),
        check_vma=False,
    )
```

```python
from functools import partial

import jax
import jax.numpy as jnp
from jax import lax
from jax.experimental import pallas as pl
from jax.experimental.pallas import tpu as pltpu
from jax.sharding import Mesh
from jax.sharding import PartitionSpec as P

SP = ("sp_0", "sp_1", "sp_2")
SP_TP = ("sp_0", "sp_1", "sp_2", "tp")

EPS = 1e-06
F32 = jnp.float32
BF16 = jnp.bfloat16

TOK = 256
BLK = 64
NB = TOK // BLK
LANES = 128
TILES = 6
STATE_ROWS = TILES * 64
PAY_ROWS = STATE_ROWS + 16


def dot(a, b):
    return lax.dot_general(a, b, (((1,), (0,)), ((), ())), preferred_element_type=F32)


def dot_t(a, b):
    return lax.dot_general(a, b, (((1,), (1,)), ((), ())), preferred_element_type=F32)


def silu(x):
    return x / (1.0 + jnp.exp(-x))


def local_kernel(
    nf_hbm, nh_hbm, ex_hbm, nq_hbm, v_hbm, wf_hbm, wh_hbm, wq_hbm, w_hbm, pay_ref, out_ref, qr_ref,
    w_ref, nf_ref, nh_ref, ex_ref, nq_ref, v_ref, wf_ref, wh_ref, wq_ref, sems,
):
    sources = (nf_hbm, nh_hbm, ex_hbm, nq_hbm, v_hbm, wf_hbm, wh_hbm, wq_hbm, w_hbm)
    targets = (nf_ref, nh_ref, ex_ref, nq_ref, v_ref, wf_ref, wh_ref, wq_ref, w_ref)
    copies = [
        pltpu.make_async_copy(a, b, sems.at[i]) for i, (a, b) in enumerate(zip(sources, targets))
    ]
    for copy in copies:
        copy.start()
    for copy in copies[:-1]:
        copy.wait()
    ex = jnp.transpose(jnp.concatenate([ex_ref[0], ex_ref[1]], axis=0))
    ri = lax.broadcasted_iota(jnp.int32, (TOK, TOK), 0)
    ci = lax.broadcasted_iota(jnp.int32, (TOK, TOK), 1)
    same = (ri // BLK) == (ci // BLK)
    tri = (same & (ci <= ri), same & (ci >= ri))
    ones = tuple(jnp.where(t, 1.0, 0.0).astype(BF16) for t in tri)
    lane = lax.broadcasted_iota(jnp.int32, (1, LANES), 1)
    low = lane < 64
    low2 = (lax.broadcasted_iota(jnp.int32, (1, 2 * LANES), 1) % LANES) < 64
    decays = [None] * (2 * TILES)

    def prepare(tile, q_raw, f_raw, rooms, extra):
        q = silu(q_raw.astype(F32)).reshape(NB, BLK, LANES)
        qi, ki, ke, qr, ends = [], [], [], [], []
        for d in range(2):
            opening = rooms[d] / (1.0 + jnp.exp(f_raw[d].astype(F32)))
            ld = jnp.log(1.0 - opening) + extra
            hi = ld.astype(BF16)
            lo = (ld - hi.astype(F32)).astype(BF16)
            both = dot(ones[d], jnp.concatenate([hi, lo], axis=1))
            inside = (both[:, :LANES] + both[:, LANES:]).reshape(NB, BLK, LANES)
            opening = opening.reshape(NB, BLK, LANES)
            edge = BLK - 1 if d == 0 else 0
            end = [inside[b, edge : edge + 1, :] for b in range(NB)]
            start = [None] * NB
            run = jnp.zeros((1, LANES), F32)
            for b in range(NB) if d == 0 else reversed(range(NB)):
                start[b] = run
                run = run + end[b]
            decays[d * TILES + tile] = jnp.exp(run)
            start4 = jnp.stack(start, axis=0)
            end4 = jnp.stack(end, axis=0)
            qi.append((q * jnp.exp(inside)).reshape(TOK, LANES))
            qr.append((q * jnp.exp(inside + start4)).reshape(TOK, LANES).astype(BF16))
            ki.append((opening * jnp.exp(-inside)).reshape(TOK, LANES))
            ke.append((opening * jnp.exp(end4 - inside)).reshape(TOK, LANES).astype(BF16))
            ends.append([jnp.exp(e) for e in end])
        qr_ref[tile] = jnp.concatenate(qr, axis=1)
        return qi, ki, jnp.concatenate(ke, axis=1), ends

    def block_states(tile, kv, ends):
        states = [[None, None] for _ in range(NB)]
        for d in range(2):
            run = jnp.zeros((64, LANES), F32)
            for b in range(NB) if d == 0 else reversed(range(NB)):
                states[b][d] = run
                run = run * ends[d][b] + kv[b * 64 : b * 64 + 64, d * LANES : (d + 1) * LANES]
            pay_ref[d, tile * 64 : tile * 64 + 64, :] = run.astype(BF16)
        return [jnp.concatenate(s, axis=1) for s in states]

    def transposed(v):
        return jnp.transpose(v.astype(F32))

    def spread(vt):
        return jnp.where(same, jnp.concatenate([vt] * NB, axis=0), 0.0).astype(BF16)

    def scores(qi, ki):
        total = jnp.where(tri[0], dot_t(qi[0].astype(BF16), ki[0].astype(BF16)), 0.0)
        total = total + jnp.where(tri[1], dot_t(qi[1].astype(BF16), ki[1].astype(BF16)), 0.0)
        return total.astype(BF16)

    for p in range(2):
        cols = slice(p * LANES, (p + 1) * LANES)
        v = v_ref[:, 0, cols]
        extra = jnp.where(low, ex[:, 2 * p : 2 * p + 1], ex[:, 2 * p + 1 : 2 * p + 2])
        qi, ki, ke, ends = prepare(
            p, nq_ref[:, cols], (nf_ref[0, :, cols], nf_ref[1, :, cols]),
            (nh_ref[0:1, cols], nh_ref[1:2, cols]), extra,
        )
        vt = transposed(v)
        kv = jnp.where(low2, dot(spread(vt[:64]), ke), dot(spread(vt[64:]), ke))
        states = block_states(p, kv, ends)
        q_cat = jnp.concatenate([x.astype(BF16) for x in qi], axis=1)
        parts = []
        for b in range(NB):
            s = jnp.concatenate(
                [jnp.where(low2, states[b], 0.0), jnp.where(low2, 0.0, states[b])], axis=0
            )
            parts.append(dot_t(q_cat[b * BLK : (b + 1) * BLK], s.astype(BF16)))
        first = dot(scores(qi, [jnp.where(low, k, 0.0) for k in ki]), v)
        second = dot(scores(qi, [jnp.where(low, 0.0, k) for k in ki]), v)
        out_ref[p] = jnp.where(low, first, second) + jnp.concatenate(parts, axis=0)

    for p in range(2):
        v = v_ref[:, 1, p * LANES : (p + 1) * LANES]
        vt = transposed(v)
        inner, q_cats, head_states = [], [], []
        for i in range(2):
            h = 2 * p + i
            cols = slice(h * LANES, (h + 1) * LANES)
            qi, ki, ke, ends = prepare(
                2 + h, wq_ref[:, cols], (wf_ref[0, :, cols], wf_ref[1, :, cols]),
                (wh_ref[0:1, cols], wh_ref[1:2, cols]), ex[:, 4 + h : 5 + h],
            )
            kv = dot(spread(vt[i * 64 : i * 64 + 64]), ke)
            head_states.append(block_states(2 + h, kv, ends))
            q_cats.append(jnp.concatenate([x.astype(BF16) for x in qi], axis=1))
            inner.append(dot(scores(qi, ki), v))
        parts = []
        for b in range(NB):
            s = jnp.concatenate([head_states[0][b], head_states[1][b]], axis=0).astype(BF16)
            rows = slice(b * BLK, (b + 1) * BLK)
            parts.append(
                jnp.where(low, dot_t(q_cats[0][rows], s), dot_t(q_cats[1][rows], s))
            )
        out_ref[2 + p] = jnp.where(low, inner[0], inner[1]) + jnp.concatenate(parts, axis=0)

    for d in range(2):
        pay_ref[d, STATE_ROWS:, :] = packed(decays[d * TILES : (d + 1) * TILES])
    copies[-1].wait()


def packed(rows):
    dec = jnp.concatenate(rows + [jnp.zeros((8 - TILES, LANES), F32)], axis=0)
    high = dec.astype(BF16).astype(F32)
    return jnp.concatenate([high, dec - high], axis=0).astype(BF16)


def unpacked(rows):
    rows = rows.astype(F32)
    return rows[:8] + rows[8:]


def pair_kernel(pieces_ref, pay_ref):
    core = lax.axis_index("sp_2")
    first, second = pieces_ref[core, core], pieces_ref[1 - core, core]
    d0, d1 = unpacked(first[STATE_ROWS:]), unpacked(second[STATE_ROWS:])
    for t in range(TILES):
        rows = slice(t * 64, t * 64 + 64)
        total = first[rows].astype(F32) * d1[t : t + 1] + second[rows].astype(F32)
        pay_ref[rows, :] = total.astype(BF16)
    both = d0 * d1
    pay_ref[STATE_ROWS:, :] = packed([both[:TILES]])


def level_kernel(count, axis, last, *refs):
    pieces, refs = refs[:count], refs[count:]
    backward = lax.axis_index("sp_2") == 1
    here = lax.axis_index(axis)
    if last:
        carry_s, carry_d, in_ref = refs
    else:
        s_ref, d_ref, pay_ref = refs
    far = jnp.where(backward, count - 1 - here, here)
    dec = [unpacked(p[STATE_ROWS:, :]) for p in pieces]

    def chosen(values, k):
        return jnp.where(backward, values[(count - k) % count], values[k])

    steps = [chosen(dec, k) for k in range(count)]
    mine_d = jnp.ones((8, LANES), F32)
    for k in range(1, count):
        mine_d = mine_d * jnp.where(far >= k, steps[k], 1.0)
    total_d = steps[0]
    for k in range(1, count):
        total_d = total_d * steps[k]
    for t in range(TILES):
        rows = slice(t * 64, t * 64 + 64)
        states = [p[rows, :].astype(F32) for p in pieces]
        ordered = [chosen(states, k) for k in range(count)]
        row = slice(t, t + 1)
        mine = jnp.zeros((64, LANES), F32)
        for k in range(count - 1, 0, -1):
            mine = jnp.where(far >= k, mine * steps[k][row] + ordered[k], mine)
        if last:
            in_ref[rows, :] = (mine * carry_d[row, :] + carry_s[rows, :]).astype(BF16)
            continue
        run = mine * steps[0][row] + ordered[0]
        for k in range(count - 1, 0, -1):
            run = jnp.where(far < k, run * steps[k][row] + ordered[k], run)
        s_ref[rows, :] = mine
        pay_ref[rows, :] = run.astype(BF16)
    if not last:
        d_ref[...] = mine_d
        pay_ref[STATE_ROWS:, :] = packed([total_d[:TILES]])


def from_each(x, axis, tiles=None):
    count = lax.axis_size(axis)
    return [
        lax.ppermute(x if tiles is None else tiles[j], axis, [(i, (i + j) % count) for i in range(count)])
        for j in range(1, count)
    ]


VMEM = pl.BlockSpec(memory_space=pltpu.VMEM)
HBM = pl.BlockSpec(memory_space=pltpu.HBM)


def in_hbm(x):
    return pltpu.with_memory_space_constraint(x, pltpu.HBM)


def small_call(kernel, name, shapes, *arrays, scratch=()):
    return pl.pallas_call(
        kernel,
        out_shape=shapes,
        in_specs=[VMEM] * len(arrays),
        out_specs=jax.tree.map(lambda _: VMEM, shapes),
        scratch_shapes=scratch,
        compiler_params=pltpu.CompilerParams(vmem_limit_bytes=8 * 2**20),
        name=name,
    )(*arrays)


def entering_states(payload):
    states = jax.ShapeDtypeStruct((STATE_ROWS, LANES), F32)
    decays = jax.ShapeDtypeStruct((8, LANES), F32)
    half = jax.ShapeDtypeStruct((PAY_ROWS, LANES), BF16)
    pieces = lax.all_gather(payload, "sp_2")
    chip = small_call(pair_kernel, "pair", half, pieces)
    s, d, row = small_call(
        partial(level_kernel, lax.axis_size("sp_1"), "sp_1", False), "level_1", (states, decays, half),
        chip, *from_each(chip, "sp_1"),
    )
    entering = small_call(
        partial(level_kernel, lax.axis_size("sp_0"), "sp_0", True), "level_0",
        jax.ShapeDtypeStruct((STATE_ROWS, LANES), BF16), row, *from_each(row, "sp_0"), s, d,
    )
    return lax.all_gather(entering, "sp_2"), pieces


def mix_kernel(out_ref, qr_ref, in_ref, pieces_ref, gate_ref, gain_ref, *refs):
    *tile_refs, mixed_ref = refs
    low = lax.broadcasted_iota(jnp.int32, (1, LANES), 1) < 64
    low2 = (lax.broadcasted_iota(jnp.int32, (1, 2 * LANES), 1) % LANES) < 64

    core = lax.axis_index("sp_2")
    gain = jnp.concatenate([gain_ref[...], gain_ref[...]], axis=1)
    dec = [unpacked(pieces_ref[d, d, STATE_ROWS:, :]) for d in range(2)]

    def entering(tile):
        rows = slice(tile * 64, tile * 64 + 64)
        parts = []
        for d in range(2):
            chip = in_ref[d, rows, :].astype(F32)
            past = chip * dec[d][tile : tile + 1] + pieces_ref[d, d, rows, :].astype(F32)
            parts.append(jnp.where(core == d, chip, past))
        return jnp.concatenate(parts, axis=1)

    zero = jnp.zeros((64, 2 * LANES), F32)
    for u in range(4):
        if u < 2:
            s = entering(u)
            s = jnp.concatenate([jnp.where(low2, s, 0.0), jnp.where(low2, 0.0, s)], axis=0)
            o = dot_t(qr_ref[u], s.astype(BF16))
        else:
            t = 2 + 2 * (u - 2)
            o = dot_t(qr_ref[t], jnp.concatenate([entering(t), zero], axis=0).astype(BF16))
            o = o + dot_t(qr_ref[t + 1], jnp.concatenate([zero, entering(t + 1)], axis=0).astype(BF16))
        o = o + out_ref[u]
        square = o * o
        first = jnp.sum(jnp.where(low, square, 0.0), axis=-1, keepdims=True)
        second = jnp.sum(jnp.where(low, 0.0, square), axis=-1, keepdims=True)
        scale = lax.rsqrt(jnp.where(low, first, second) * (1.0 / 64) + EPS)
        c = (u % 2) * LANES
        gate = silu(gate_ref[:, u // 2, c : c + LANES].astype(F32))
        mixed = o * scale * gain * gate
        mixed_ref[:, u * LANES : (u + 1) * LANES] = mixed.astype(BF16)
    count, rows = len(tile_refs), tile_refs[0].shape[0]
    for j, tile_ref in enumerate(tile_refs):
        place = lax.rem(lax.axis_index("tp") + j, count)
        tile_ref[...] = mixed_ref[pl.ds(place * rows, rows), :]


def earlier_in_block(size, rows, axis):
    ri = lax.broadcasted_iota(jnp.int32, (size, size), 0)
    ci = lax.broadcasted_iota(jnp.int32, (size, size), 1)
    first, second = (ri, ci) if axis == 0 else (ci, ri)
    same = (ri // rows) == (ci // rows)
    return same, same & (first < second)


def slots_of(col, row, capacity, rows, axis):
    same, earlier = earlier_in_block(col[0].shape[0], rows, axis)
    own = row if axis == 0 else col
    other = col if axis == 0 else row

    def count(hit):
        return jnp.sum(jnp.where(hit, 1.0, 0.0), axis=axis, keepdims=True).astype(jnp.int32)

    rank0 = count((own[0] == other[0]) & earlier)
    rank1 = count((own[1] == other[1]) & earlier) + count((own[1] == other[0]) & same)
    return own[0] * capacity + rank0, own[1] * capacity + rank1


def route_kernel(
    experts, capacity, copies, x0_ref, x1_ref, x2_ref, x3_ref, w_ref, stream_ref, gain_ref,
    routes_ref, score_ref, res_ref, buf_ref, pick_ref, table_ref,
):
    rows, width = res_ref.shape
    here = lax.axis_index("tp")
    own = pl.ds(here * rows, rows)
    residual = stream_ref[own, :].astype(F32)
    span = 2 * LANES
    for j, x_ref in enumerate((x0_ref, x1_ref, x2_ref, x3_ref)):
        source = lax.rem(here + copies - j, copies)
        for g in range(2):
            part = x_ref[:, g * span : (g + 1) * span]
            residual = residual + dot(part, w_ref[g, pl.ds(source * span, span), :])
    res_ref[...] = residual
    mean = jnp.mean(residual * residual, axis=-1, keepdims=True)
    norm = (residual * lax.rsqrt(mean + EPS) * gain_ref[...]).astype(BF16)
    table = jnp.concatenate(
        [routes_ref[...].astype(F32), score_ref[...], jnp.zeros((4, routes_ref.shape[1]), F32)], axis=0
    )
    table_ref[...] = jnp.transpose(table)
    table = table_ref[own, :]
    table_t = jnp.transpose(table)
    col = [table[:, k : k + 1].astype(jnp.int32) for k in range(2)]
    row = [table_t[k : k + 1, :].astype(jnp.int32) for k in range(2)]
    slots = slots_of(col, row, capacity, rows, 1)
    s0, s1 = table[:, 2:3], table[:, 3:4]
    weights = (1.0 / (1.0 + jnp.exp(s1 - s0)), 1.0 / (1.0 + jnp.exp(s0 - s1)))
    j = lax.broadcasted_iota(jnp.int32, (rows, experts * copies * capacity), 1)
    code = (j // (copies * capacity)) * capacity + j % capacity
    hits = [code == slot for slot in slots]
    pick = jnp.where(hits[0], weights[0], 0.0) + jnp.where(hits[1], weights[1], 0.0)
    high = pick.astype(BF16)
    pick_ref[:rows, :] = high
    pick_ref[rows:, :] = (pick - high.astype(F32)).astype(BF16)
    chosen = jnp.transpose(jnp.where(hits[0] | hits[1], 1.0, 0.0)).astype(BF16)
    buf_ref[...] = dot(chosen, norm).astype(BF16)


def final_kernel(pick_ref, back_ref, res_ref, o_ref):
    rows = res_ref.shape[0]
    both = dot(pick_ref[...], back_ref[...])
    o_ref[...] = (res_ref[...] + both[:rows] + both[rows:]).astype(BF16)


def local(
    stream,
    narrow_query_weight,
    wide_query_weight,
    value_rows_heads,
    output_gate_logits,
    narrow_forget_logits,
    wide_forget_logits,
    narrow_forget_headroom,
    wide_forget_headroom,
    extra_log_decay,
    per_head_norm_gain,
    mixer_output_weight,
    feedforward_norm_gain,
    expert_gate_matrix,
    expert_up_matrix,
    expert_down_matrix,
    routes,
    router_scores_chosen,
):
    local_inputs = (
        narrow_forget_logits, narrow_forget_headroom, extra_log_decay.transpose(1, 2, 0),
        narrow_query_weight, value_rows_heads, wide_forget_logits, wide_forget_headroom,
        wide_query_weight,
    )
    payload, inner, q_run, mixer_weight = pl.pallas_call(
        local_kernel,
        out_shape=(
            jax.ShapeDtypeStruct((2, PAY_ROWS, LANES), BF16),
            jax.ShapeDtypeStruct((4, TOK, LANES), F32),
            jax.ShapeDtypeStruct((TILES, TOK, 2 * LANES), BF16),
            pltpu.VMEM(mixer_output_weight.shape, BF16),
        ),
        in_specs=[HBM] * 9,
        out_specs=(VMEM,) * 4,
        scratch_shapes=[pltpu.VMEM(x.shape, x.dtype) for x in local_inputs]
        + [pltpu.SemaphoreType.DMA((9,))],
        compiler_params=pltpu.CompilerParams(vmem_limit_bytes=16 * 2**20),
        name="local_mixer",
    )(*map(in_hbm, local_inputs), in_hbm(mixer_output_weight))
    entering, pieces = entering_states(payload)
    tp = lax.axis_size("tp")
    rows = TOK // tp
    tiles = small_call(
        mix_kernel, "mix", (jax.ShapeDtypeStruct((rows, 4 * LANES), BF16),) * tp, inner, q_run,
        entering, pieces, output_gate_logits, per_head_norm_gain.reshape(1, 64),
        scratch=[pltpu.VMEM((TOK, 4 * LANES), BF16)],
    )
    width = stream.shape[1]
    experts = lax.axis_size(SP)
    capacity = max(2, 2 * routes.shape[1] * rows // experts)
    slots = experts * tp * capacity
    arrived = [tiles[0]] + from_each(None, "tp", tiles)
    residual, buffers, pick = pl.pallas_call(
        partial(route_kernel, experts, capacity, tp),
        out_shape=(
            jax.ShapeDtypeStruct((rows, width), F32),
            jax.ShapeDtypeStruct((slots, width), BF16),
            jax.ShapeDtypeStruct((2 * rows, slots), BF16),
        ),
        in_specs=[VMEM] * 9,
        out_specs=(VMEM,) * 3,
        scratch_shapes=[pltpu.VMEM((TOK, 8), F32)],
        compiler_params=pltpu.CompilerParams(vmem_limit_bytes=24 * 2**20),
        name="project_and_route",
    )(
        *arrived, mixer_weight, stream, feedforward_norm_gain.reshape(1, width),
        routes.T, router_scores_chosen.T,
    )
    tokens = lax.all_to_all(buffers, SP_TP, 0, 0, tiled=True)
    gate = jnp.dot(tokens, expert_gate_matrix[0], preferred_element_type=F32)
    up = jnp.dot(tokens, expert_up_matrix[0], preferred_element_type=F32)
    hidden = (jax.nn.silu(gate) * up).astype(BF16)
    part = jnp.dot(hidden, expert_down_matrix[0], preferred_element_type=F32).astype(BF16)
    back = lax.all_to_all(part, SP_TP, 0, 0, tiled=True)
    col = width // 4
    return pl.pallas_call(
        final_kernel,
        grid=(4,),
        in_specs=[
            pl.BlockSpec((2 * rows, slots), lambda i: (0, 0)),
            pl.BlockSpec((slots, col), lambda i: (0, i)),
            pl.BlockSpec((rows, col), lambda i: (0, i)),
        ],
        out_specs=pl.BlockSpec((rows, col), lambda i: (0, i)),
        out_shape=jax.ShapeDtypeStruct((rows, width), BF16),
        compiler_params=pltpu.CompilerParams(vmem_limit_bytes=12 * 2**20),
        name="combine",
    )(pick, back, residual)


def solution(mesh):
    torus = Mesh(mesh.devices.reshape(4, 4, 2, mesh.shape["tp"]), ("sp_0", "sp_1", "sp_2", "tp"))
    return jax.shard_map(
        local,
        mesh=torus,
        in_specs=(
            P(SP, None),
            P(SP, "tp"),
            P(SP, "tp"),
            P(SP, None, "tp"),
            P(SP, None, "tp"),
            P(None, SP, "tp"),
            P(None, SP, "tp"),
            P(None, "tp"),
            P(None, "tp"),
            P(SP, None, "tp"),
            P(),
            P(),
            P(),
            P(SP, None, "tp"),
            P(SP, None, "tp"),
            P(SP, "tp", None),
            P(SP, None),
            P(SP, None),
        ),
        out_specs=P(SP_TP, None),
        check_vma=False,
    )
```

```python
from functools import partial

import jax
import jax.numpy as jnp
from jax import lax
from jax.experimental import pallas as pl
from jax.experimental.pallas import tpu as pltpu
from jax.sharding import Mesh
from jax.sharding import PartitionSpec as P

SP = ("sp_0", "sp_1", "sp_2")
SP_TP = ("sp_0", "sp_1", "sp_2", "tp")

EPS = 1e-06
F32 = jnp.float32
BF16 = jnp.bfloat16

TOK = 256
BLK = 64
NB = TOK // BLK
LANES = 128
TILES = 6
STATE_ROWS = TILES * 64
PAY_ROWS = STATE_ROWS + 16


def dot(a, b):
    return lax.dot_general(a, b, (((1,), (0,)), ((), ())), preferred_element_type=F32)


def dot_t(a, b):
    return lax.dot_general(a, b, (((1,), (1,)), ((), ())), preferred_element_type=F32)


def silu(x):
    return x / (1.0 + jnp.exp(-x))


def copied(sources, targets, sems):
    copies = [
        pltpu.make_async_copy(a, b, sems.at[i]) for i, (a, b) in enumerate(zip(sources, targets))
    ]
    for copy in copies:
        copy.start()
    return copies


class Tiles:
    def __init__(self, ex_ref):
        ri = lax.broadcasted_iota(jnp.int32, (TOK, TOK), 0)
        ci = lax.broadcasted_iota(jnp.int32, (TOK, TOK), 1)
        self.same = (ri // BLK) == (ci // BLK)
        self.tri = (self.same & (ci <= ri), self.same & (ci >= ri))
        self.ones = tuple(jnp.where(t, 1.0, 0.0).astype(BF16) for t in self.tri)
        self.low = lax.broadcasted_iota(jnp.int32, (1, LANES), 1) < 64
        self.low2 = (lax.broadcasted_iota(jnp.int32, (1, 2 * LANES), 1) % LANES) < 64
        self.ex = jnp.transpose(jnp.concatenate([ex_ref[0], ex_ref[1]], axis=0))

    def extra(self, tile):
        if tile >= 2:
            return self.ex[:, tile + 2 : tile + 3]
        return jnp.where(
            self.low, self.ex[:, 2 * tile : 2 * tile + 1], self.ex[:, 2 * tile + 1 : 2 * tile + 2]
        )

    def decayed(self, tile, d, f_raw, room):
        opening = room / (1.0 + jnp.exp(f_raw.astype(F32)))
        ld = jnp.log(1.0 - opening) + self.extra(tile)
        hi = ld.astype(BF16)
        lo = (ld - hi.astype(F32)).astype(BF16)
        both = dot(self.ones[d], jnp.concatenate([hi, lo], axis=1))
        inside = (both[:, :LANES] + both[:, LANES:]).reshape(NB, BLK, LANES)
        edge = BLK - 1 if d == 0 else 0
        end = [inside[b, edge : edge + 1, :] for b in range(NB)]
        start = [None] * NB
        run = jnp.zeros((1, LANES), F32)
        for b in range(NB) if d == 0 else reversed(range(NB)):
            start[b] = run
            run = run + end[b]
        opening = opening.reshape(NB, BLK, LANES)
        ke = (opening * jnp.exp(jnp.stack(end, axis=0) - inside)).reshape(TOK, LANES).astype(BF16)
        return opening, inside, [jnp.exp(e) for e in end], jnp.stack(start, axis=0), run, ke

    def block_values(self, tile, v, ke):
        vt = jnp.transpose(v.astype(F32))

        def spread(part):
            return jnp.where(self.same, jnp.concatenate([part] * NB, axis=0), 0.0).astype(BF16)

        if tile >= 2:
            half = (tile % 2) * 64
            return dot(spread(vt[half : half + 64]), ke)
        return jnp.where(self.low2, dot(spread(vt[:64]), ke), dot(spread(vt[64:]), ke))

    def swept(self, kv, ends):
        states = [[None, None] for _ in range(NB)]
        closing = []
        for d in range(2):
            run = jnp.zeros((64, LANES), F32)
            for b in range(NB) if d == 0 else reversed(range(NB)):
                states[b][d] = run
                run = run * ends[d][b] + kv[b * 64 : b * 64 + 64, d * LANES : (d + 1) * LANES]
            closing.append(run)
        return [jnp.concatenate(s, axis=1) for s in states], closing


def place_of(tile):
    if tile < 2:
        return slice(tile * LANES, (tile + 1) * LANES), slice(tile * LANES, (tile + 1) * LANES)
    h = tile - 2
    return slice(h * LANES, (h + 1) * LANES), slice(h // 2 * LANES, (h // 2 + 1) * LANES)


def states_kernel(
    nf_hbm, nh_hbm, ex_hbm, v_hbm, wf_hbm, wh_hbm, pay_ref, nf_ref, nh_ref, ex_ref, v_ref, wf_ref,
    wh_ref, sems,
):
    copies = copied(
        (nf_hbm, nh_hbm, ex_hbm, v_hbm, wf_hbm, wh_hbm),
        (nf_ref, nh_ref, ex_ref, v_ref, wf_ref, wh_ref),
        sems,
    )
    for copy in copies[:4]:
        copy.wait()
    tiles = Tiles(ex_ref)
    decays = [[], []]
    for tile in range(TILES):
        if tile == 2:
            for copy in copies[4:]:
                copy.wait()
        cols, v_cols = place_of(tile)
        f_ref, h_ref = (nf_ref, nh_ref) if tile < 2 else (wf_ref, wh_ref)
        ke, ends = [], []
        for d in range(2):
            _, _, end, _, total, k = tiles.decayed(tile, d, f_ref[d, :, cols], h_ref[d : d + 1, cols])
            ke.append(k)
            ends.append(end)
            decays[d].append(jnp.exp(total))
        kv = tiles.block_values(tile, v_ref[:, 0 if tile < 2 else 1, v_cols], jnp.concatenate(ke, axis=1))
        _, closing = tiles.swept(kv, ends)
        for d in range(2):
            pay_ref[d, tile * 64 : tile * 64 + 64, :] = closing[d].astype(BF16)
    for d in range(2):
        pay_ref[d, STATE_ROWS:, :] = packed(decays[d])


def narrow_kernel(
    nf_hbm, nh_hbm, ex_hbm, v_hbm, nq_hbm, w_hbm, after_ref, out_ref, qr_ref, w_ref,
    nf_ref, nh_ref, ex_ref, v_ref, nq_ref, sems,
):
    del after_ref
    copies = copied(
        (nf_hbm, nh_hbm, ex_hbm, v_hbm, nq_hbm, w_hbm), (nf_ref, nh_ref, ex_ref, v_ref, nq_ref, w_ref), sems
    )
    for copy in copies[:-1]:
        copy.wait()
    own_outputs(0, nf_ref, nh_ref, ex_ref, v_ref, nq_ref, out_ref, qr_ref)
    copies[-1].wait()


def wide_kernel(
    wf_hbm, wh_hbm, ex_hbm, v_hbm, wq_hbm, after_ref, out_ref, qr_ref, token_ref,
    wf_ref, wh_ref, ex_ref, v_ref, wq_ref, sems,
):
    del after_ref
    for copy in copied(
        (wf_hbm, wh_hbm, ex_hbm, v_hbm, wq_hbm), (wf_ref, wh_ref, ex_ref, v_ref, wq_ref), sems
    ):
        copy.wait()
    own_outputs(1, wf_ref, wh_ref, ex_ref, v_ref, wq_ref, out_ref, qr_ref)
    token_ref[...] = jnp.zeros(token_ref.shape, F32)


def own_outputs(group, f_ref, h_ref, ex_ref, v_ref, q_ref, out_ref, qr_ref):
    tiles = Tiles(ex_ref)
    low, low2 = tiles.low, tiles.low2

    def prepare(tile):
        cols, v_cols = place_of(tile)
        q = silu(q_ref[:, cols].astype(F32)).reshape(NB, BLK, LANES)
        qi, ki, ke, qr, ends = [], [], [], [], []
        for d in range(2):
            opening, inside, end, start, _, k = tiles.decayed(
                tile, d, f_ref[d, :, cols], h_ref[d : d + 1, cols]
            )
            qi.append((q * jnp.exp(inside)).reshape(TOK, LANES))
            qr.append((q * jnp.exp(inside + start)).reshape(TOK, LANES).astype(BF16))
            ki.append((opening * jnp.exp(-inside)).reshape(TOK, LANES))
            ke.append(k)
            ends.append(end)
        qr_ref[tile - 2 * group] = jnp.concatenate(qr, axis=1)
        v = v_ref[:, group, v_cols]
        states, _ = tiles.swept(tiles.block_values(tile, v, jnp.concatenate(ke, axis=1)), ends)
        return qi, ki, states, v

    def scores(qi, ki):
        total = jnp.where(tiles.tri[0], dot_t(qi[0].astype(BF16), ki[0].astype(BF16)), 0.0)
        total = total + jnp.where(tiles.tri[1], dot_t(qi[1].astype(BF16), ki[1].astype(BF16)), 0.0)
        return total.astype(BF16)

    def joined(qi):
        return jnp.concatenate([x.astype(BF16) for x in qi], axis=1)

    for p in range(2) if group == 0 else ():
        qi, ki, states, v = prepare(p)
        q_cat = joined(qi)
        parts = []
        for b in range(NB):
            s = jnp.concatenate(
                [jnp.where(low2, states[b], 0.0), jnp.where(low2, 0.0, states[b])], axis=0
            )
            parts.append(dot_t(q_cat[b * BLK : (b + 1) * BLK], s.astype(BF16)))
        first = dot(scores(qi, [jnp.where(low, k, 0.0) for k in ki]), v)
        second = dot(scores(qi, [jnp.where(low, 0.0, k) for k in ki]), v)
        out_ref[p] = jnp.where(low, first, second) + jnp.concatenate(parts, axis=0)

    for p in range(2) if group == 1 else ():
        inner, q_cats, head_states = [], [], []
        for tile in (2 + 2 * p, 3 + 2 * p):
            qi, ki, states, v = prepare(tile)
            head_states.append(states)
            q_cats.append(joined(qi))
            inner.append(dot(scores(qi, ki), v))
        parts = []
        for b in range(NB):
            s = jnp.concatenate([head_states[0][b], head_states[1][b]], axis=0).astype(BF16)
            rows = slice(b * BLK, (b + 1) * BLK)
            parts.append(
                jnp.where(low, dot_t(q_cats[0][rows], s), dot_t(q_cats[1][rows], s))
            )
        out_ref[p] = jnp.where(low, inner[0], inner[1]) + jnp.concatenate(parts, axis=0)


def packed(rows):
    dec = jnp.concatenate(rows + [jnp.zeros((8 - TILES, LANES), F32)], axis=0)
    high = dec.astype(BF16).astype(F32)
    return jnp.concatenate([high, dec - high], axis=0).astype(BF16)


def unpacked(rows):
    rows = rows.astype(F32)
    return rows[:8] + rows[8:]


def pair_kernel(pieces_ref, pay_ref):
    core = lax.axis_index("sp_2")
    first, second = pieces_ref[core, core], pieces_ref[1 - core, core]
    d0, d1 = unpacked(first[STATE_ROWS:]), unpacked(second[STATE_ROWS:])
    for t in range(TILES):
        rows = slice(t * 64, t * 64 + 64)
        total = first[rows].astype(F32) * d1[t : t + 1] + second[rows].astype(F32)
        pay_ref[rows, :] = total.astype(BF16)
    both = d0 * d1
    pay_ref[STATE_ROWS:, :] = packed([both[:TILES]])


def level_kernel(count, axis, last, *refs):
    if not last:
        refs = refs[1:]
    pieces, refs = refs[:count], refs[count:]
    backward = lax.axis_index("sp_2") == 1
    here = lax.axis_index(axis)
    if last:
        carry_s, carry_d, in_ref = refs
    else:
        s_ref, d_ref, pay_ref = refs
    far = jnp.where(backward, count - 1 - here, here)
    dec = [unpacked(p[STATE_ROWS:, :]) for p in pieces]

    def chosen(values, k):
        return jnp.where(backward, values[(count - k) % count], values[k])

    steps = [chosen(dec, k) for k in range(count)]
    mine_d = jnp.ones((8, LANES), F32)
    for k in range(1, count):
        mine_d = mine_d * jnp.where(far >= k, steps[k], 1.0)
    total_d = steps[0]
    for k in range(1, count):
        total_d = total_d * steps[k]
    for t in range(TILES):
        rows = slice(t * 64, t * 64 + 64)
        states = [p[rows, :].astype(F32) for p in pieces]
        ordered = [chosen(states, k) for k in range(count)]
        row = slice(t, t + 1)
        mine = jnp.zeros((64, LANES), F32)
        for k in range(count - 1, 0, -1):
            mine = jnp.where(far >= k, mine * steps[k][row] + ordered[k], mine)
        if last:
            in_ref[rows, :] = (mine * carry_d[row, :] + carry_s[rows, :]).astype(BF16)
            continue
        run = mine * steps[0][row] + ordered[0]
        for k in range(count - 1, 0, -1):
            run = jnp.where(far < k, run * steps[k][row] + ordered[k], run)
        s_ref[rows, :] = mine
        pay_ref[rows, :] = run.astype(BF16)
    if not last:
        d_ref[...] = mine_d
        pay_ref[STATE_ROWS:, :] = packed([total_d[:TILES]])


def from_each(x, axis, tiles=None):
    count = lax.axis_size(axis)
    return [
        lax.ppermute(x if tiles is None else tiles[j], axis, [(i, (i + j) % count) for i in range(count)])
        for j in range(1, count)
    ]


VMEM = pl.BlockSpec(memory_space=pltpu.VMEM)
HBM = pl.BlockSpec(memory_space=pltpu.HBM)


def in_hbm(x):
    return pltpu.with_memory_space_constraint(x, pltpu.HBM)


def small_call(kernel, name, shapes, *arrays, scratch=()):
    return pl.pallas_call(
        kernel,
        out_shape=shapes,
        in_specs=[VMEM] * len(arrays),
        out_specs=jax.tree.map(lambda _: VMEM, shapes),
        scratch_shapes=scratch,
        compiler_params=pltpu.CompilerParams(vmem_limit_bytes=8 * 2**20),
        name=name,
    )(*arrays)


def mix_kernel(n_out_ref, n_qr_ref, w_out_ref, w_qr_ref, in_ref, pieces_ref, gate_ref, gain_ref, *refs):
    *tile_refs, mixed_ref = refs
    low = lax.broadcasted_iota(jnp.int32, (1, LANES), 1) < 64
    low2 = (lax.broadcasted_iota(jnp.int32, (1, 2 * LANES), 1) % LANES) < 64

    core = lax.axis_index("sp_2")
    gain = jnp.concatenate([gain_ref[...], gain_ref[...]], axis=1)
    dec = [unpacked(pieces_ref[d, d, STATE_ROWS:, :]) for d in range(2)]

    def entering(tile):
        rows = slice(tile * 64, tile * 64 + 64)
        parts = []
        for d in range(2):
            chip = in_ref[d, rows, :].astype(F32)
            past = chip * dec[d][tile : tile + 1] + pieces_ref[d, d, rows, :].astype(F32)
            parts.append(jnp.where(core == d, chip, past))
        return jnp.concatenate(parts, axis=1)

    zero = jnp.zeros((64, 2 * LANES), F32)
    for u in range(4):
        if u < 2:
            s = entering(u)
            s = jnp.concatenate([jnp.where(low2, s, 0.0), jnp.where(low2, 0.0, s)], axis=0)
            o = dot_t(n_qr_ref[u], s.astype(BF16)) + n_out_ref[u]
        else:
            t = 2 + 2 * (u - 2)
            o = w_out_ref[u - 2] + dot_t(w_qr_ref[t - 2], jnp.concatenate([entering(t), zero], axis=0).astype(BF16))
            o = o + dot_t(w_qr_ref[t - 1], jnp.concatenate([zero, entering(t + 1)], axis=0).astype(BF16))
        square = o * o
        first = jnp.sum(jnp.where(low, square, 0.0), axis=-1, keepdims=True)
        second = jnp.sum(jnp.where(low, 0.0, square), axis=-1, keepdims=True)
        scale = lax.rsqrt(jnp.where(low, first, second) * (1.0 / 64) + EPS)
        c = (u % 2) * LANES
        gate = silu(gate_ref[:, u // 2, c : c + LANES].astype(F32))
        mixed = o * scale * gain * gate
        mixed_ref[:, u * LANES : (u + 1) * LANES] = mixed.astype(BF16)
    count, rows = len(tile_refs), tile_refs[0].shape[0]
    for j, tile_ref in enumerate(tile_refs):
        place = lax.rem(lax.axis_index("tp") + j, count)
        tile_ref[...] = mixed_ref[pl.ds(place * rows, rows), :]


def earlier_in_block(size, rows, axis):
    ri = lax.broadcasted_iota(jnp.int32, (size, size), 0)
    ci = lax.broadcasted_iota(jnp.int32, (size, size), 1)
    first, second = (ri, ci) if axis == 0 else (ci, ri)
    same = (ri // rows) == (ci // rows)
    return same, same & (first < second)


def slots_of(col, row, capacity, rows, axis):
    same, earlier = earlier_in_block(col[0].shape[0], rows, axis)
    own = row if axis == 0 else col
    other = col if axis == 0 else row

    def count(hit):
        return jnp.sum(jnp.where(hit, 1.0, 0.0), axis=axis, keepdims=True).astype(jnp.int32)

    rank0 = count((own[0] == other[0]) & earlier)
    rank1 = count((own[1] == other[1]) & earlier) + count((own[1] == other[0]) & same)
    return own[0] * capacity + rank0, own[1] * capacity + rank1


def route_kernel(
    experts, capacity, copies, x0_ref, x1_ref, x2_ref, x3_ref, w_ref, stream_ref, gain_ref,
    routes_ref, score_ref, res_ref, buf_ref, pick_ref, table_ref,
):
    rows, width = res_ref.shape
    here = lax.axis_index("tp")
    own = pl.ds(here * rows, rows)
    residual = stream_ref[own, :].astype(F32)
    span = 2 * LANES
    for j, x_ref in enumerate((x0_ref, x1_ref, x2_ref, x3_ref)):
        source = lax.rem(here + copies - j, copies)
        for g in range(2):
            part = x_ref[:, g * span : (g + 1) * span]
            residual = residual + dot(part, w_ref[g, pl.ds(source * span, span), :])
    res_ref[...] = residual
    mean = jnp.mean(residual * residual, axis=-1, keepdims=True)
    norm = (residual * lax.rsqrt(mean + EPS) * gain_ref[...]).astype(BF16)
    table = jnp.concatenate(
        [routes_ref[...].astype(F32), score_ref[...], jnp.zeros((4, routes_ref.shape[1]), F32)], axis=0
    )
    table_ref[...] = jnp.transpose(table)
    table = table_ref[own, :]
    table_t = jnp.transpose(table)
    col = [table[:, k : k + 1].astype(jnp.int32) for k in range(2)]
    row = [table_t[k : k + 1, :].astype(jnp.int32) for k in range(2)]
    slots = slots_of(col, row, capacity, rows, 1)
    s0, s1 = table[:, 2:3], table[:, 3:4]
    weights = (1.0 / (1.0 + jnp.exp(s1 - s0)), 1.0 / (1.0 + jnp.exp(s0 - s1)))
    j = lax.broadcasted_iota(jnp.int32, (rows, experts * copies * capacity), 1)
    code = (j // (copies * capacity)) * capacity + j % capacity
    hits = [code == slot for slot in slots]
    pick = jnp.where(hits[0], weights[0], 0.0) + jnp.where(hits[1], weights[1], 0.0)
    high = pick.astype(BF16)
    pick_ref[:rows, :] = high
    pick_ref[rows:, :] = (pick - high.astype(F32)).astype(BF16)
    chosen = jnp.transpose(jnp.where(hits[0] | hits[1], 1.0, 0.0)).astype(BF16)
    buf_ref[...] = dot(chosen, norm).astype(BF16)


def final_kernel(pick_ref, back_ref, res_ref, o_ref):
    rows = res_ref.shape[0]
    both = dot(pick_ref[...], back_ref[...])
    o_ref[...] = (res_ref[...] + both[:rows] + both[rows:]).astype(BF16)


def local(
    stream,
    narrow_query_weight,
    wide_query_weight,
    value_rows_heads,
    output_gate_logits,
    narrow_forget_logits,
    wide_forget_logits,
    narrow_forget_headroom,
    wide_forget_headroom,
    extra_log_decay,
    per_head_norm_gain,
    mixer_output_weight,
    feedforward_norm_gain,
    expert_gate_matrix,
    expert_up_matrix,
    expert_down_matrix,
    routes,
    router_scores_chosen,
):
    nf, wf = in_hbm(narrow_forget_logits), in_hbm(wide_forget_logits)
    nh, wh = in_hbm(narrow_forget_headroom), in_hbm(wide_forget_headroom)
    nq, wq = in_hbm(narrow_query_weight), in_hbm(wide_query_weight)
    extra, values = in_hbm(extra_log_decay.transpose(1, 2, 0)), in_hbm(value_rows_heads)

    def from_hbm(kernel, name, inputs, shapes, vmem, after=(), kept=0, flops=0):
        buffered = inputs[: len(inputs) - kept]
        return pl.pallas_call(
            kernel,
            out_shape=shapes,
            in_specs=[HBM] * len(inputs) + [VMEM] * len(after),
            out_specs=jax.tree.map(lambda _: VMEM, shapes),
            scratch_shapes=[pltpu.VMEM(x.shape, x.dtype) for x in buffered]
            + [pltpu.SemaphoreType.DMA((len(inputs),))],
            compiler_params=pltpu.CompilerParams(vmem_limit_bytes=vmem * 2**20),
            cost_estimate=pl.CostEstimate(
                flops=flops, bytes_accessed=3 * 2**20, transcendentals=2 * 10**6
            ),
            name=name,
        )(*inputs, *after)

    payload = from_hbm(
        states_kernel, "local_states", (nf, nh, extra, values, wf, wh),
        jax.ShapeDtypeStruct((2, PAY_ROWS, LANES), BF16), 12, flops=10**9,
    )
    states = jax.ShapeDtypeStruct((STATE_ROWS, LANES), F32)
    decays = jax.ShapeDtypeStruct((8, LANES), F32)
    half = jax.ShapeDtypeStruct((PAY_ROWS, LANES), BF16)
    own = jax.ShapeDtypeStruct((2, TOK, LANES), F32)

    def queries(count):
        return jax.ShapeDtypeStruct((count, TOK, 2 * LANES), BF16)

    pieces = lax.all_gather(payload, "sp_2")
    chip = small_call(pair_kernel, "pair", half, pieces)
    chips = [chip, *from_each(chip, "sp_1")]
    wide, wide_q, token = from_hbm(
        wide_kernel, "wide_outputs", (wf, wh, extra, values, wq), (own, queries(4), decays), 20,
        after=(chip,), flops=3 * 10**9,
    )
    s, d, row = small_call(
        partial(level_kernel, lax.axis_size("sp_1"), "sp_1", False), "level_1", (states, decays, half),
        token, *chips,
    )
    rows_ = [row, *from_each(row, "sp_0")]
    narrow, narrow_q, mixer_weight = from_hbm(
        narrow_kernel, "narrow_outputs", (nf, nh, extra, values, nq, in_hbm(mixer_output_weight)),
        (own, queries(2), pltpu.VMEM(mixer_output_weight.shape, BF16)), 20, after=(d,), kept=1,
        flops=3 * 10**9,
    )
    entering = small_call(
        partial(level_kernel, lax.axis_size("sp_0"), "sp_0", True), "level_0",
        jax.ShapeDtypeStruct((STATE_ROWS, LANES), BF16), *rows_, s, d,
    )
    entering = lax.all_gather(entering, "sp_2")
    tp = lax.axis_size("tp")
    rows = TOK // tp
    tiles = small_call(
        mix_kernel, "mix", (jax.ShapeDtypeStruct((rows, 4 * LANES), BF16),) * tp, narrow, narrow_q,
        wide, wide_q, entering, pieces, output_gate_logits, per_head_norm_gain.reshape(1, 64),
        scratch=[pltpu.VMEM((TOK, 4 * LANES), BF16)],
    )
    width = stream.shape[1]
    experts = lax.axis_size(SP)
    capacity = max(2, 2 * routes.shape[1] * rows // experts)
    slots = experts * tp * capacity
    arrived = [tiles[0]] + from_each(None, "tp", tiles)
    residual, buffers, pick = pl.pallas_call(
        partial(route_kernel, experts, capacity, tp),
        out_shape=(
            jax.ShapeDtypeStruct((rows, width), F32),
            jax.ShapeDtypeStruct((slots, width), BF16),
            jax.ShapeDtypeStruct((2 * rows, slots), BF16),
        ),
        in_specs=[VMEM] * 9,
        out_specs=(VMEM,) * 3,
        scratch_shapes=[pltpu.VMEM((TOK, 8), F32)],
        compiler_params=pltpu.CompilerParams(vmem_limit_bytes=24 * 2**20),
        name="project_and_route",
    )(
        *arrived, mixer_weight, stream, feedforward_norm_gain.reshape(1, width),
        routes.T, router_scores_chosen.T,
    )
    tokens = lax.all_to_all(buffers, SP_TP, 0, 0, tiled=True)
    gate = jnp.dot(tokens, expert_gate_matrix[0], preferred_element_type=F32)
    up = jnp.dot(tokens, expert_up_matrix[0], preferred_element_type=F32)
    hidden = (jax.nn.silu(gate) * up).astype(BF16)
    part = jnp.dot(hidden, expert_down_matrix[0], preferred_element_type=F32).astype(BF16)
    back = lax.all_to_all(part, SP_TP, 0, 0, tiled=True)
    return pl.pallas_call(
        final_kernel,
        in_specs=[VMEM] * 3,
        out_specs=VMEM,
        out_shape=jax.ShapeDtypeStruct((rows, width), BF16),
        compiler_params=pltpu.CompilerParams(vmem_limit_bytes=12 * 2**20),
        name="combine",
    )(pick, back, residual)


def solution(mesh):
    torus = Mesh(mesh.devices.reshape(4, 4, 2, mesh.shape["tp"]), ("sp_0", "sp_1", "sp_2", "tp"))
    return jax.shard_map(
        local,
        mesh=torus,
        in_specs=(
            P(SP, None),
            P(SP, "tp"),
            P(SP, "tp"),
            P(SP, None, "tp"),
            P(SP, None, "tp"),
            P(None, SP, "tp"),
            P(None, SP, "tp"),
            P(None, "tp"),
            P(None, "tp"),
            P(SP, None, "tp"),
            P(),
            P(),
            P(),
            P(SP, None, "tp"),
            P(SP, None, "tp"),
            P(SP, "tp", None),
            P(SP, None),
            P(SP, None),
        ),
        out_specs=P(SP_TP, None),
        check_vma=False,
    )
```

```python
from functools import partial

import jax
import jax.numpy as jnp
from jax import lax
from jax.experimental import pallas as pl
from jax.experimental.pallas import tpu as pltpu
from jax.sharding import Mesh
from jax.sharding import PartitionSpec as P

SP = ("sp_0", "sp_1", "sp_2")
SP_TP = ("sp_0", "sp_1", "sp_2", "tp")

EPS = 1e-06
F32 = jnp.float32
BF16 = jnp.bfloat16

TOK = 256
BLK = 64
NB = TOK // BLK
LANES = 128
TILES = 6
STATE_ROWS = TILES * 64
PAY_ROWS = STATE_ROWS + 16


def dot(a, b):
    return lax.dot_general(a, b, (((1,), (0,)), ((), ())), preferred_element_type=F32)


def dot_t(a, b):
    return lax.dot_general(a, b, (((1,), (1,)), ((), ())), preferred_element_type=F32)


def silu(x):
    return x / (1.0 + jnp.exp(-x))


def copied(sources, targets, sems):
    copies = [
        pltpu.make_async_copy(a, b, sems.at[i]) for i, (a, b) in enumerate(zip(sources, targets))
    ]
    for copy in copies:
        copy.start()
    return copies


class Tiles:
    def __init__(self, ex_ref):
        ri = lax.broadcasted_iota(jnp.int32, (TOK, TOK), 0)
        ci = lax.broadcasted_iota(jnp.int32, (TOK, TOK), 1)
        self.same = (ri // BLK) == (ci // BLK)
        self.tri = (self.same & (ci <= ri), self.same & (ci >= ri))
        self.ones = tuple(jnp.where(t, 1.0, 0.0).astype(BF16) for t in self.tri)
        self.low = lax.broadcasted_iota(jnp.int32, (1, LANES), 1) < 64
        self.low2 = (lax.broadcasted_iota(jnp.int32, (1, 2 * LANES), 1) % LANES) < 64
        self.ex = jnp.transpose(jnp.concatenate([ex_ref[0], ex_ref[1]], axis=0))

    def extra(self, tile):
        if tile >= 2:
            return self.ex[:, tile + 2 : tile + 3]
        return jnp.where(
            self.low, self.ex[:, 2 * tile : 2 * tile + 1], self.ex[:, 2 * tile + 1 : 2 * tile + 2]
        )

    def decayed(self, tile, d, f_raw, room):
        opening = room / (1.0 + jnp.exp(f_raw.astype(F32)))
        ld = jnp.log(1.0 - opening) + self.extra(tile)
        hi = ld.astype(BF16)
        lo = (ld - hi.astype(F32)).astype(BF16)
        both = dot(self.ones[d], jnp.concatenate([hi, lo], axis=1))
        inside = (both[:, :LANES] + both[:, LANES:]).reshape(NB, BLK, LANES)
        edge = BLK - 1 if d == 0 else 0
        end = [inside[b, edge : edge + 1, :] for b in range(NB)]
        start = [None] * NB
        run = jnp.zeros((1, LANES), F32)
        for b in range(NB) if d == 0 else reversed(range(NB)):
            start[b] = run
            run = run + end[b]
        opening = opening.reshape(NB, BLK, LANES)
        ke = (opening * jnp.exp(jnp.stack(end, axis=0) - inside)).reshape(TOK, LANES).astype(BF16)
        return opening, inside, [jnp.exp(e) for e in end], jnp.stack(start, axis=0), run, ke

    def block_values(self, tile, v, ke):
        vt = jnp.transpose(v.astype(F32))

        def spread(part):
            return jnp.where(self.same, jnp.concatenate([part] * NB, axis=0), 0.0).astype(BF16)

        if tile >= 2:
            half = (tile % 2) * 64
            return dot(spread(vt[half : half + 64]), ke)
        return jnp.where(self.low2, dot(spread(vt[:64]), ke), dot(spread(vt[64:]), ke))

    def swept(self, kv, ends):
        states = [[None, None] for _ in range(NB)]
        closing = []
        for d in range(2):
            run = jnp.zeros((64, LANES), F32)
            for b in range(NB) if d == 0 else reversed(range(NB)):
                states[b][d] = run
                run = run * ends[d][b] + kv[b * 64 : b * 64 + 64, d * LANES : (d + 1) * LANES]
            closing.append(run)
        return [jnp.concatenate(s, axis=1) for s in states], closing


def place_of(tile):
    if tile < 2:
        return slice(tile * LANES, (tile + 1) * LANES), slice(tile * LANES, (tile + 1) * LANES)
    h = tile - 2
    return slice(h * LANES, (h + 1) * LANES), slice(h // 2 * LANES, (h // 2 + 1) * LANES)


def states_kernel(
    nf_hbm, nh_hbm, ex_hbm, v_hbm, wf_hbm, wh_hbm, pay_ref, nf_ref, nh_ref, ex_ref, v_ref, wf_ref,
    wh_ref, sems,
):
    copies = copied(
        (nf_hbm, nh_hbm, ex_hbm, v_hbm, wf_hbm, wh_hbm),
        (nf_ref, nh_ref, ex_ref, v_ref, wf_ref, wh_ref),
        sems,
    )
    for copy in copies[:4]:
        copy.wait()
    tiles = Tiles(ex_ref)
    decays = [[], []]
    for tile in range(TILES):
        if tile == 2:
            for copy in copies[4:]:
                copy.wait()
        cols, v_cols = place_of(tile)
        f_ref, h_ref = (nf_ref, nh_ref) if tile < 2 else (wf_ref, wh_ref)
        ke, ends = [], []
        for d in range(2):
            _, _, end, _, total, k = tiles.decayed(tile, d, f_ref[d, :, cols], h_ref[d : d + 1, cols])
            ke.append(k)
            ends.append(end)
            decays[d].append(jnp.exp(total))
        kv = tiles.block_values(tile, v_ref[:, 0 if tile < 2 else 1, v_cols], jnp.concatenate(ke, axis=1))
        _, closing = tiles.swept(kv, ends)
        for d in range(2):
            pay_ref[d, tile * 64 : tile * 64 + 64, :] = closing[d].astype(BF16)
    for d in range(2):
        pay_ref[d, STATE_ROWS:, :] = packed(decays[d])


def narrow_kernel(
    nf_hbm, nh_hbm, ex_hbm, v_hbm, nq_hbm, w_hbm, after_ref, out_ref, qr_ref, w_ref,
    nf_ref, nh_ref, ex_ref, v_ref, nq_ref, sems,
):
    del after_ref
    copies = copied(
        (nf_hbm, nh_hbm, ex_hbm, v_hbm, nq_hbm, w_hbm), (nf_ref, nh_ref, ex_ref, v_ref, nq_ref, w_ref), sems
    )
    for copy in copies[:-1]:
        copy.wait()
    own_outputs(0, nf_ref, nh_ref, ex_ref, v_ref, nq_ref, out_ref, qr_ref)
    copies[-1].wait()


def wide_kernel(
    wf_hbm, wh_hbm, ex_hbm, v_hbm, wq_hbm, after_ref, out_ref, qr_ref, token_ref,
    wf_ref, wh_ref, ex_ref, v_ref, wq_ref, sems,
):
    del after_ref
    for copy in copied(
        (wf_hbm, wh_hbm, ex_hbm, v_hbm, wq_hbm), (wf_ref, wh_ref, ex_ref, v_ref, wq_ref), sems
    ):
        copy.wait()
    own_outputs(1, wf_ref, wh_ref, ex_ref, v_ref, wq_ref, out_ref, qr_ref)
    token_ref[...] = jnp.zeros(token_ref.shape, F32)


def own_outputs(group, f_ref, h_ref, ex_ref, v_ref, q_ref, out_ref, qr_ref):
    tiles = Tiles(ex_ref)
    low, low2 = tiles.low, tiles.low2

    def prepare(tile):
        cols, v_cols = place_of(tile)
        q = silu(q_ref[:, cols].astype(F32)).reshape(NB, BLK, LANES)
        qi, ki, ke, qr, ends = [], [], [], [], []
        for d in range(2):
            opening, inside, end, start, _, k = tiles.decayed(
                tile, d, f_ref[d, :, cols], h_ref[d : d + 1, cols]
            )
            qi.append((q * jnp.exp(inside)).reshape(TOK, LANES))
            qr.append((q * jnp.exp(inside + start)).reshape(TOK, LANES).astype(BF16))
            ki.append((opening * jnp.exp(-inside)).reshape(TOK, LANES))
            ke.append(k)
            ends.append(end)
        qr_ref[tile - 2 * group] = jnp.concatenate(qr, axis=1)
        v = v_ref[:, group, v_cols]
        states, _ = tiles.swept(tiles.block_values(tile, v, jnp.concatenate(ke, axis=1)), ends)
        return qi, ki, states, v

    def scores(qi, ki):
        total = jnp.where(tiles.tri[0], dot_t(qi[0].astype(BF16), ki[0].astype(BF16)), 0.0)
        total = total + jnp.where(tiles.tri[1], dot_t(qi[1].astype(BF16), ki[1].astype(BF16)), 0.0)
        return total.astype(BF16)

    def joined(qi):
        return jnp.concatenate([x.astype(BF16) for x in qi], axis=1)

    for p in range(2) if group == 0 else ():
        qi, ki, states, v = prepare(p)
        q_cat = joined(qi)
        parts = []
        for b in range(NB):
            s = jnp.concatenate(
                [jnp.where(low2, states[b], 0.0), jnp.where(low2, 0.0, states[b])], axis=0
            )
            parts.append(dot_t(q_cat[b * BLK : (b + 1) * BLK], s.astype(BF16)))
        first = dot(scores(qi, [jnp.where(low, k, 0.0) for k in ki]), v)
        second = dot(scores(qi, [jnp.where(low, 0.0, k) for k in ki]), v)
        out_ref[p] = jnp.where(low, first, second) + jnp.concatenate(parts, axis=0)

    for p in range(2) if group == 1 else ():
        inner, q_cats, head_states = [], [], []
        for tile in (2 + 2 * p, 3 + 2 * p):
            qi, ki, states, v = prepare(tile)
            head_states.append(states)
            q_cats.append(joined(qi))
            inner.append(dot(scores(qi, ki), v))
        parts = []
        for b in range(NB):
            s = jnp.concatenate([head_states[0][b], head_states[1][b]], axis=0).astype(BF16)
            rows = slice(b * BLK, (b + 1) * BLK)
            parts.append(
                jnp.where(low, dot_t(q_cats[0][rows], s), dot_t(q_cats[1][rows], s))
            )
        out_ref[p] = jnp.where(low, inner[0], inner[1]) + jnp.concatenate(parts, axis=0)


def packed(rows):
    dec = jnp.concatenate(rows + [jnp.zeros((8 - TILES, LANES), F32)], axis=0)
    high = dec.astype(BF16).astype(F32)
    return jnp.concatenate([high, dec - high], axis=0).astype(BF16)


def unpacked(rows):
    rows = rows.astype(F32)
    return rows[:8] + rows[8:]


def pair_kernel(pieces_ref, pay_ref):
    core = lax.axis_index("sp_2")
    first, second = pieces_ref[core, core], pieces_ref[1 - core, core]
    d0, d1 = unpacked(first[STATE_ROWS:]), unpacked(second[STATE_ROWS:])
    for t in range(TILES):
        rows = slice(t * 64, t * 64 + 64)
        total = first[rows].astype(F32) * d1[t : t + 1] + second[rows].astype(F32)
        pay_ref[rows, :] = total.astype(BF16)
    both = d0 * d1
    pay_ref[STATE_ROWS:, :] = packed([both[:TILES]])


def level_kernel(count, axis, last, *refs):
    if not last:
        refs = refs[1:]
    pieces, refs = refs[:count], refs[count:]
    backward = lax.axis_index("sp_2") == 1
    here = lax.axis_index(axis)
    if last:
        carry_s, carry_d, in_ref = refs
    else:
        s_ref, d_ref, pay_ref = refs
    far = jnp.where(backward, count - 1 - here, here)
    dec = [unpacked(p[STATE_ROWS:, :]) for p in pieces]

    def chosen(values, k):
        return jnp.where(backward, values[(count - k) % count], values[k])

    steps = [chosen(dec, k) for k in range(count)]
    mine_d = jnp.ones((8, LANES), F32)
    for k in range(1, count):
        mine_d = mine_d * jnp.where(far >= k, steps[k], 1.0)
    total_d = steps[0]
    for k in range(1, count):
        total_d = total_d * steps[k]
    for t in range(TILES):
        rows = slice(t * 64, t * 64 + 64)
        states = [p[rows, :].astype(F32) for p in pieces]
        ordered = [chosen(states, k) for k in range(count)]
        row = slice(t, t + 1)
        mine = jnp.zeros((64, LANES), F32)
        for k in range(count - 1, 0, -1):
            mine = jnp.where(far >= k, mine * steps[k][row] + ordered[k], mine)
        if last:
            in_ref[rows, :] = (mine * carry_d[row, :] + carry_s[rows, :]).astype(BF16)
            continue
        run = mine * steps[0][row] + ordered[0]
        for k in range(count - 1, 0, -1):
            run = jnp.where(far < k, run * steps[k][row] + ordered[k], run)
        s_ref[rows, :] = mine
        pay_ref[rows, :] = run.astype(BF16)
    if not last:
        d_ref[...] = mine_d
        pay_ref[STATE_ROWS:, :] = packed([total_d[:TILES]])


def from_each(x, axis, tiles=None):
    count = lax.axis_size(axis)
    return [
        lax.ppermute(x if tiles is None else tiles[j], axis, [(i, (i + j) % count) for i in range(count)])
        for j in range(1, count)
    ]


VMEM = pl.BlockSpec(memory_space=pltpu.VMEM)
HBM = pl.BlockSpec(memory_space=pltpu.HBM)


def in_hbm(x):
    return pltpu.with_memory_space_constraint(x, pltpu.HBM)


def small_call(kernel, name, shapes, *arrays, scratch=(), flops=0):
    return pl.pallas_call(
        kernel,
        out_shape=shapes,
        in_specs=[VMEM] * len(arrays),
        out_specs=jax.tree.map(lambda _: VMEM, shapes),
        scratch_shapes=scratch,
        cost_estimate=pl.CostEstimate(flops=flops, bytes_accessed=2**20, transcendentals=0),
        compiler_params=pltpu.CompilerParams(vmem_limit_bytes=8 * 2**20),
        name=name,
    )(*arrays)


def mix_kernel(n_out_ref, n_qr_ref, w_out_ref, w_qr_ref, in_ref, pieces_ref, gate_ref, gain_ref, *refs):
    *tile_refs, mixed_ref = refs
    low = lax.broadcasted_iota(jnp.int32, (1, LANES), 1) < 64
    low2 = (lax.broadcasted_iota(jnp.int32, (1, 2 * LANES), 1) % LANES) < 64

    core = lax.axis_index("sp_2")
    gain = jnp.concatenate([gain_ref[...], gain_ref[...]], axis=1)
    dec = [unpacked(pieces_ref[d, d, STATE_ROWS:, :]) for d in range(2)]

    def entering(tile):
        rows = slice(tile * 64, tile * 64 + 64)
        parts = []
        for d in range(2):
            chip = in_ref[d, rows, :].astype(F32)
            past = chip * dec[d][tile : tile + 1] + pieces_ref[d, d, rows, :].astype(F32)
            parts.append(jnp.where(core == d, chip, past))
        return jnp.concatenate(parts, axis=1)

    zero = jnp.zeros((64, 2 * LANES), F32)
    for u in range(4):
        if u < 2:
            s = entering(u)
            s = jnp.concatenate([jnp.where(low2, s, 0.0), jnp.where(low2, 0.0, s)], axis=0)
            o = dot_t(n_qr_ref[u], s.astype(BF16)) + n_out_ref[u]
        else:
            t = 2 + 2 * (u - 2)
            o = w_out_ref[u - 2] + dot_t(w_qr_ref[t - 2], jnp.concatenate([entering(t), zero], axis=0).astype(BF16))
            o = o + dot_t(w_qr_ref[t - 1], jnp.concatenate([zero, entering(t + 1)], axis=0).astype(BF16))
        square = o * o
        first = jnp.sum(jnp.where(low, square, 0.0), axis=-1, keepdims=True)
        second = jnp.sum(jnp.where(low, 0.0, square), axis=-1, keepdims=True)
        scale = lax.rsqrt(jnp.where(low, first, second) * (1.0 / 64) + EPS)
        c = (u % 2) * LANES
        gate = silu(gate_ref[:, u // 2, c : c + LANES].astype(F32))
        mixed = o * scale * gain * gate
        mixed_ref[:, u * LANES : (u + 1) * LANES] = mixed.astype(BF16)
    count, rows = len(tile_refs), tile_refs[0].shape[0]
    for j, tile_ref in enumerate(tile_refs):
        place = lax.rem(lax.axis_index("tp") + j, count)
        tile_ref[...] = mixed_ref[pl.ds(place * rows, rows), :]


def earlier_in_block(size, rows, axis):
    ri = lax.broadcasted_iota(jnp.int32, (size, size), 0)
    ci = lax.broadcasted_iota(jnp.int32, (size, size), 1)
    first, second = (ri, ci) if axis == 0 else (ci, ri)
    same = (ri // rows) == (ci // rows)
    return same, same & (first < second)


def slots_of(col, row, capacity, rows, axis):
    same, earlier = earlier_in_block(col[0].shape[0], rows, axis)
    own = row if axis == 0 else col
    other = col if axis == 0 else row

    def count(hit):
        return jnp.sum(jnp.where(hit, 1.0, 0.0), axis=axis, keepdims=True).astype(jnp.int32)

    rank0 = count((own[0] == other[0]) & earlier)
    rank1 = count((own[1] == other[1]) & earlier) + count((own[1] == other[0]) & same)
    return own[0] * capacity + rank0, own[1] * capacity + rank1


def picks_kernel(experts, capacity, copies, routes_ref, score_ref, after_ref, pick_ref, chosen_ref, table_ref):
    del after_ref
    rows = chosen_ref.shape[1]
    table = jnp.concatenate(
        [routes_ref[...].astype(F32), score_ref[...], jnp.zeros((4, routes_ref.shape[1]), F32)], axis=0
    )
    table_ref[...] = jnp.transpose(table)
    table = table_ref[pl.ds(lax.axis_index("tp") * rows, rows), :]
    table_t = jnp.transpose(table)
    col = [table[:, k : k + 1].astype(jnp.int32) for k in range(2)]
    row = [table_t[k : k + 1, :].astype(jnp.int32) for k in range(2)]
    slots = slots_of(col, row, capacity, rows, 1)
    s0, s1 = table[:, 2:3], table[:, 3:4]
    weights = (1.0 / (1.0 + jnp.exp(s1 - s0)), 1.0 / (1.0 + jnp.exp(s0 - s1)))
    j = lax.broadcasted_iota(jnp.int32, (rows, experts * copies * capacity), 1)
    code = (j // (copies * capacity)) * capacity + j % capacity
    hits = [code == slot for slot in slots]
    pick = jnp.where(hits[0], weights[0], 0.0) + jnp.where(hits[1], weights[1], 0.0)
    high = pick.astype(BF16)
    pick_ref[:rows, :] = high
    pick_ref[rows:, :] = (pick - high.astype(F32)).astype(BF16)
    j = lax.broadcasted_iota(jnp.int32, (rows, experts * capacity), 1)
    chosen = jnp.where((j == slots[0]) | (j == slots[1]), 1.0, 0.0)
    chosen_ref[...] = jnp.transpose(chosen).astype(BF16)


def route_kernel(
    x0_ref, x1_ref, x2_ref, x3_ref, w_ref, stream_ref, gain_ref, chosen_ref, res_ref, buf_ref
):
    rows, width = res_ref.shape
    experts, copies, capacity, _ = buf_ref.shape
    here = lax.axis_index("tp")
    residual = stream_ref[pl.ds(here * rows, rows), :].astype(F32)
    span = 2 * LANES
    for j, x_ref in enumerate((x0_ref, x1_ref, x2_ref, x3_ref)):
        source = lax.rem(here + copies - j, copies)
        for g in range(2):
            part = x_ref[:, g * span : (g + 1) * span]
            residual = residual + dot(part, w_ref[g, pl.ds(source * span, span), :])
    res_ref[...] = residual
    mean = jnp.mean(residual * residual, axis=-1, keepdims=True)
    norm = (residual * lax.rsqrt(mean + EPS) * gain_ref[...]).astype(BF16)
    sent = dot(chosen_ref[...], norm).astype(BF16).reshape(experts, capacity, width)
    for t in range(copies):
        buf_ref[:, t] = sent


def final_kernel(pick_ref, back_ref, res_ref, o_ref):
    rows = res_ref.shape[0]
    both = dot(pick_ref[...], back_ref[...])
    o_ref[...] = (res_ref[...] + both[:rows] + both[rows:]).astype(BF16)


def local(
    stream,
    narrow_query_weight,
    wide_query_weight,
    value_rows_heads,
    output_gate_logits,
    narrow_forget_logits,
    wide_forget_logits,
    narrow_forget_headroom,
    wide_forget_headroom,
    extra_log_decay,
    per_head_norm_gain,
    mixer_output_weight,
    feedforward_norm_gain,
    expert_gate_matrix,
    expert_up_matrix,
    expert_down_matrix,
    routes,
    router_scores_chosen,
):
    nf, wf = in_hbm(narrow_forget_logits), in_hbm(wide_forget_logits)
    nh, wh = in_hbm(narrow_forget_headroom), in_hbm(wide_forget_headroom)
    nq, wq = in_hbm(narrow_query_weight), in_hbm(wide_query_weight)
    extra, values = in_hbm(extra_log_decay.transpose(1, 2, 0)), in_hbm(value_rows_heads)

    def from_hbm(kernel, name, inputs, shapes, vmem, after=(), kept=0, flops=0):
        buffered = inputs[: len(inputs) - kept]
        return pl.pallas_call(
            kernel,
            out_shape=shapes,
            in_specs=[HBM] * len(inputs) + [VMEM] * len(after),
            out_specs=jax.tree.map(lambda _: VMEM, shapes),
            scratch_shapes=[pltpu.VMEM(x.shape, x.dtype) for x in buffered]
            + [pltpu.SemaphoreType.DMA((len(inputs),))],
            compiler_params=pltpu.CompilerParams(vmem_limit_bytes=vmem * 2**20),
            cost_estimate=pl.CostEstimate(
                flops=flops, bytes_accessed=3 * 2**20, transcendentals=2 * 10**6
            ),
            name=name,
        )(*inputs, *after)

    payload = from_hbm(
        states_kernel, "local_states", (nf, nh, extra, values, wf, wh),
        jax.ShapeDtypeStruct((2, PAY_ROWS, LANES), BF16), 12, flops=10**9,
    )
    states = jax.ShapeDtypeStruct((STATE_ROWS, LANES), F32)
    decays = jax.ShapeDtypeStruct((8, LANES), F32)
    half = jax.ShapeDtypeStruct((PAY_ROWS, LANES), BF16)
    own = jax.ShapeDtypeStruct((2, TOK, LANES), F32)

    def queries(count):
        return jax.ShapeDtypeStruct((count, TOK, 2 * LANES), BF16)

    pieces = lax.all_gather(payload, "sp_2")
    chip = small_call(pair_kernel, "pair", half, pieces)
    chips = [chip, *from_each(chip, "sp_1")]
    wide, wide_q, token = from_hbm(
        wide_kernel, "wide_outputs", (wf, wh, extra, values, wq), (own, queries(4), decays), 20,
        after=(chip,), flops=3 * 10**9,
    )
    s, d, row = small_call(
        partial(level_kernel, lax.axis_size("sp_1"), "sp_1", False), "level_1", (states, decays, half),
        token, *chips,
    )
    rows_ = [row, *from_each(row, "sp_0")]
    narrow, narrow_q, mixer_weight = from_hbm(
        narrow_kernel, "narrow_outputs", (nf, nh, extra, values, nq, in_hbm(mixer_output_weight)),
        (own, queries(2), pltpu.VMEM(mixer_output_weight.shape, BF16)), 20, after=(d,), kept=1,
        flops=3 * 10**9,
    )
    entering = small_call(
        partial(level_kernel, lax.axis_size("sp_0"), "sp_0", True), "level_0",
        jax.ShapeDtypeStruct((STATE_ROWS, LANES), BF16), *rows_, s, d,
    )
    entering = lax.all_gather(entering, "sp_2")
    tp = lax.axis_size("tp")
    rows = TOK // tp
    tiles = small_call(
        mix_kernel, "mix", (jax.ShapeDtypeStruct((rows, 4 * LANES), BF16),) * tp, narrow, narrow_q,
        wide, wide_q, entering, pieces, output_gate_logits, per_head_norm_gain.reshape(1, 64),
        scratch=[pltpu.VMEM((TOK, 4 * LANES), BF16)],
    )
    width = stream.shape[1]
    experts = lax.axis_size(SP)
    capacity = max(2, 2 * routes.shape[1] * rows // experts)
    slots = experts * tp * capacity
    pick, chosen = small_call(
        partial(picks_kernel, experts, capacity, tp), "picks",
        (
            jax.ShapeDtypeStruct((2 * rows, slots), BF16),
            jax.ShapeDtypeStruct((experts * capacity, rows), BF16),
        ),
        routes.T, router_scores_chosen.T, d, scratch=[pltpu.VMEM((TOK, 8), F32)],
        flops=10**9,
    )
    arrived = [tiles[0]] + from_each(None, "tp", tiles)
    residual, buffers = pl.pallas_call(
        route_kernel,
        out_shape=(
            jax.ShapeDtypeStruct((rows, width), F32),
            jax.ShapeDtypeStruct((experts, tp, capacity, width), BF16),
        ),
        in_specs=[VMEM] * 8,
        out_specs=(VMEM,) * 2,
        compiler_params=pltpu.CompilerParams(vmem_limit_bytes=20 * 2**20),
        name="project_and_route",
    )(
        *arrived, mixer_weight, stream, feedforward_norm_gain.reshape(1, width), chosen,
    )
    buffers = buffers.reshape(slots, width)
    tokens = lax.all_to_all(buffers, SP_TP, 0, 0, tiled=True)
    gate = jnp.dot(tokens, expert_gate_matrix[0], preferred_element_type=F32)
    up = jnp.dot(tokens, expert_up_matrix[0], preferred_element_type=F32)
    hidden = (jax.nn.silu(gate) * up).astype(BF16)
    part = jnp.dot(hidden, expert_down_matrix[0], preferred_element_type=F32).astype(BF16)
    back = lax.all_to_all(part, SP_TP, 0, 0, tiled=True)
    return pl.pallas_call(
        final_kernel,
        in_specs=[VMEM] * 3,
        out_specs=VMEM,
        out_shape=jax.ShapeDtypeStruct((rows, width), BF16),
        compiler_params=pltpu.CompilerParams(vmem_limit_bytes=12 * 2**20),
        name="combine",
    )(pick, back, residual)


def solution(mesh):
    torus = Mesh(mesh.devices.reshape(4, 4, 2, mesh.shape["tp"]), ("sp_0", "sp_1", "sp_2", "tp"))
    return jax.shard_map(
        local,
        mesh=torus,
        in_specs=(
            P(SP, None),
            P(SP, "tp"),
            P(SP, "tp"),
            P(SP, None, "tp"),
            P(SP, None, "tp"),
            P(None, SP, "tp"),
            P(None, SP, "tp"),
            P(None, "tp"),
            P(None, "tp"),
            P(SP, None, "tp"),
            P(),
            P(),
            P(),
            P(SP, None, "tp"),
            P(SP, None, "tp"),
            P(SP, "tp", None),
            P(SP, None),
            P(SP, None),
        ),
        out_specs=P(SP_TP, None),
        check_vma=False,
    )
```

```python
from functools import partial

import jax
import jax.numpy as jnp
from jax import lax
from jax.experimental import pallas as pl
from jax.experimental.pallas import tpu as pltpu
from jax.sharding import Mesh
from jax.sharding import PartitionSpec as P

SP = ("sp_0", "sp_1", "sp_2")
SP_TP = ("sp_0", "sp_1", "sp_2", "tp")

EPS = 1e-06
F32 = jnp.float32
BF16 = jnp.bfloat16

TOK = 256
BLK = 64
NB = TOK // BLK
LANES = 128
TILES = 6
STATE_ROWS = TILES * 64
PAY_ROWS = STATE_ROWS + 16


def dot(a, b):
    return lax.dot_general(a, b, (((1,), (0,)), ((), ())), preferred_element_type=F32)


def dot_t(a, b):
    return lax.dot_general(a, b, (((1,), (1,)), ((), ())), preferred_element_type=F32)


def silu(x):
    return x / (1.0 + jnp.exp(-x))


def copied(sources, targets, sems):
    copies = [
        pltpu.make_async_copy(a, b, sems.at[i]) for i, (a, b) in enumerate(zip(sources, targets))
    ]
    for copy in copies:
        copy.start()
    return copies


class Tiles:
    def __init__(self, ex_ref):
        ri = lax.broadcasted_iota(jnp.int32, (TOK, TOK), 0)
        ci = lax.broadcasted_iota(jnp.int32, (TOK, TOK), 1)
        self.same = (ri // BLK) == (ci // BLK)
        self.tri = (self.same & (ci <= ri), self.same & (ci >= ri))
        ones = [jnp.where(t, 1.0, 0.0).astype(BF16) for t in self.tri]
        self.ones = [jnp.concatenate([t, t], axis=1) for t in ones]
        self.low = lax.broadcasted_iota(jnp.int32, (1, LANES), 1) < 64
        self.low2 = (lax.broadcasted_iota(jnp.int32, (1, 2 * LANES), 1) % LANES) < 64
        self.ex = jnp.transpose(jnp.concatenate([ex_ref[0], ex_ref[1]], axis=0))

    def extra(self, tile):
        if tile >= 2:
            return self.ex[:, tile + 2 : tile + 3]
        return jnp.where(
            self.low, self.ex[:, 2 * tile : 2 * tile + 1], self.ex[:, 2 * tile + 1 : 2 * tile + 2]
        )

    def decayed(self, tile, d, f_raw, room):
        opening = room / (1.0 + jnp.exp(f_raw.astype(F32)))
        ld = jnp.log(1.0 - opening) + self.extra(tile)
        hi = ld.astype(BF16)
        lo = (ld - hi.astype(F32)).astype(BF16)
        inside = dot(self.ones[d], jnp.concatenate([hi, lo], axis=0)).reshape(NB, BLK, LANES)
        edge = BLK - 1 if d == 0 else 0
        end = [inside[b, edge : edge + 1, :] for b in range(NB)]
        start = [None] * NB
        run = jnp.zeros((1, LANES), F32)
        for b in range(NB) if d == 0 else reversed(range(NB)):
            start[b] = run
            run = run + end[b]
        opening = opening.reshape(NB, BLK, LANES)
        ke = (opening * jnp.exp(jnp.stack(end, axis=0) - inside)).reshape(TOK, LANES).astype(BF16)
        return opening, inside, [jnp.exp(e) for e in end], jnp.stack(start, axis=0), run, ke

    def block_values(self, tile, v, ke):
        vt = jnp.transpose(v.astype(F32))

        def spread(part):
            return jnp.where(self.same, jnp.concatenate([part] * NB, axis=0), 0.0).astype(BF16)

        if tile >= 2:
            half = (tile % 2) * 64
            return dot(spread(vt[half : half + 64]), ke)
        return jnp.where(self.low2, dot(spread(vt[:64]), ke), dot(spread(vt[64:]), ke))

    def swept(self, kv, ends):
        states = [[None, None] for _ in range(NB)]
        closing = []
        for d in range(2):
            run = jnp.zeros((64, LANES), F32)
            for b in range(NB) if d == 0 else reversed(range(NB)):
                states[b][d] = run
                run = run * ends[d][b] + kv[b * 64 : b * 64 + 64, d * LANES : (d + 1) * LANES]
            closing.append(run)
        return [jnp.concatenate(s, axis=1) for s in states], closing


def place_of(tile):
    if tile < 2:
        return slice(tile * LANES, (tile + 1) * LANES), slice(tile * LANES, (tile + 1) * LANES)
    h = tile - 2
    return slice(h * LANES, (h + 1) * LANES), slice(h // 2 * LANES, (h // 2 + 1) * LANES)


def states_kernel(
    nf_hbm, nh_hbm, ex_hbm, v_hbm, wf_hbm, wh_hbm, pay_ref, nf_ref, nh_ref, ex_ref, v_ref, wf_ref,
    wh_ref, sems,
):
    copies = copied(
        (nf_hbm, nh_hbm, ex_hbm, v_hbm, wf_hbm, wh_hbm),
        (nf_ref, nh_ref, ex_ref, v_ref, wf_ref, wh_ref),
        sems,
    )
    for copy in copies[:4]:
        copy.wait()
    tiles = Tiles(ex_ref)
    decays = [[], []]
    for tile in range(TILES):
        if tile == 2:
            for copy in copies[4:]:
                copy.wait()
        cols, v_cols = place_of(tile)
        f_ref, h_ref = (nf_ref, nh_ref) if tile < 2 else (wf_ref, wh_ref)
        ke, ends = [], []
        for d in range(2):
            _, _, end, _, total, k = tiles.decayed(tile, d, f_ref[d, :, cols], h_ref[d : d + 1, cols])
            ke.append(k)
            ends.append(end)
            decays[d].append(jnp.exp(total))
        kv = tiles.block_values(tile, v_ref[:, 0 if tile < 2 else 1, v_cols], jnp.concatenate(ke, axis=1))
        _, closing = tiles.swept(kv, ends)
        for d in range(2):
            pay_ref[d, tile * 64 : tile * 64 + 64, :] = closing[d].astype(BF16)
    for d in range(2):
        pay_ref[d, STATE_ROWS:, :] = packed(decays[d])


def narrow_kernel(
    nf_hbm, nh_hbm, ex_hbm, v_hbm, nq_hbm, gate_hbm, w_hbm, gain_ref, after_ref, out_ref, qr_ref,
    gates_ref, w_ref, nf_ref, nh_ref, ex_ref, v_ref, nq_ref, gate_ref, sems,
):
    del after_ref
    copies = copied(
        (nf_hbm, nh_hbm, ex_hbm, v_hbm, nq_hbm, gate_hbm, w_hbm),
        (nf_ref, nh_ref, ex_ref, v_ref, nq_ref, gate_ref, w_ref), sems,
    )
    for copy in copies[:-1]:
        copy.wait()
    own_outputs(0, nf_ref, nh_ref, ex_ref, v_ref, nq_ref, out_ref, qr_ref)
    gain = jnp.concatenate([gain_ref[...], gain_ref[...]], axis=1)
    for u in range(4):
        c = (u % 2) * LANES
        gates_ref[u] = silu(gate_ref[:, u // 2, c : c + LANES].astype(F32)) * gain
    copies[-1].wait()


def wide_kernel(
    wf_hbm, wh_hbm, ex_hbm, v_hbm, wq_hbm, after_ref, out_ref, qr_ref, token_ref,
    wf_ref, wh_ref, ex_ref, v_ref, wq_ref, sems,
):
    del after_ref
    for copy in copied(
        (wf_hbm, wh_hbm, ex_hbm, v_hbm, wq_hbm), (wf_ref, wh_ref, ex_ref, v_ref, wq_ref), sems
    ):
        copy.wait()
    own_outputs(1, wf_ref, wh_ref, ex_ref, v_ref, wq_ref, out_ref, qr_ref)
    token_ref[...] = jnp.zeros(token_ref.shape, F32)


def own_outputs(group, f_ref, h_ref, ex_ref, v_ref, q_ref, out_ref, qr_ref):
    tiles = Tiles(ex_ref)
    low, low2 = tiles.low, tiles.low2

    def prepare(tile):
        cols, v_cols = place_of(tile)
        q = silu(q_ref[:, cols].astype(F32)).reshape(NB, BLK, LANES)
        qi, ki, ke, qr, ends = [], [], [], [], []
        for d in range(2):
            opening, inside, end, start, _, k = tiles.decayed(
                tile, d, f_ref[d, :, cols], h_ref[d : d + 1, cols]
            )
            qi.append((q * jnp.exp(inside)).reshape(TOK, LANES))
            qr.append((q * jnp.exp(inside + start)).reshape(TOK, LANES).astype(BF16))
            ki.append((opening * jnp.exp(-inside)).reshape(TOK, LANES))
            ke.append(k)
            ends.append(end)
        qr_ref[tile - 2 * group] = jnp.concatenate(qr, axis=1)
        v = v_ref[:, group, v_cols]
        states, _ = tiles.swept(tiles.block_values(tile, v, jnp.concatenate(ke, axis=1)), ends)
        return qi, ki, states, v

    def scores(qi, ki):
        total = jnp.where(tiles.tri[0], dot_t(qi[0].astype(BF16), ki[0].astype(BF16)), 0.0)
        total = total + jnp.where(tiles.tri[1], dot_t(qi[1].astype(BF16), ki[1].astype(BF16)), 0.0)
        return total.astype(BF16)

    def joined(qi):
        return jnp.concatenate([x.astype(BF16) for x in qi], axis=1)

    for p in range(2) if group == 0 else ():
        qi, ki, states, v = prepare(p)
        q_cat = joined(qi)
        parts = []
        for b in range(NB):
            s = jnp.concatenate(
                [jnp.where(low2, states[b], 0.0), jnp.where(low2, 0.0, states[b])], axis=0
            )
            parts.append(dot_t(q_cat[b * BLK : (b + 1) * BLK], s.astype(BF16)))
        first = dot(scores(qi, [jnp.where(low, k, 0.0) for k in ki]), v)
        second = dot(scores(qi, [jnp.where(low, 0.0, k) for k in ki]), v)
        out_ref[p] = jnp.where(low, first, second) + jnp.concatenate(parts, axis=0)

    for p in range(2) if group == 1 else ():
        inner, q_cats, head_states = [], [], []
        for tile in (2 + 2 * p, 3 + 2 * p):
            qi, ki, states, v = prepare(tile)
            head_states.append(states)
            q_cats.append(joined(qi))
            inner.append(dot(scores(qi, ki), v))
        parts = []
        for b in range(NB):
            s = jnp.concatenate([head_states[0][b], head_states[1][b]], axis=0).astype(BF16)
            rows = slice(b * BLK, (b + 1) * BLK)
            parts.append(
                jnp.where(low, dot_t(q_cats[0][rows], s), dot_t(q_cats[1][rows], s))
            )
        out_ref[p] = jnp.where(low, inner[0], inner[1]) + jnp.concatenate(parts, axis=0)


def packed(rows):
    dec = jnp.concatenate(rows + [jnp.zeros((8 - TILES, LANES), F32)], axis=0)
    high = dec.astype(BF16).astype(F32)
    return jnp.concatenate([high, dec - high], axis=0).astype(BF16)


def unpacked(rows):
    rows = rows.astype(F32)
    return rows[:8] + rows[8:]


def pair_kernel(pieces_ref, pay_ref):
    core = lax.axis_index("sp_2")
    first, second = pieces_ref[core, core], pieces_ref[1 - core, core]
    d0, d1 = unpacked(first[STATE_ROWS:]), unpacked(second[STATE_ROWS:])
    for t in range(TILES):
        rows = slice(t * 64, t * 64 + 64)
        total = first[rows].astype(F32) * d1[t : t + 1] + second[rows].astype(F32)
        pay_ref[rows, :] = total.astype(BF16)
    both = d0 * d1
    pay_ref[STATE_ROWS:, :] = packed([both[:TILES]])


def level_kernel(count, axis, last, *refs):
    if not last:
        refs = refs[1:]
    pieces, refs = refs[:count], refs[count:]
    backward = lax.axis_index("sp_2") == 1
    here = lax.axis_index(axis)
    if last:
        carry_s, carry_d, in_ref = refs
    else:
        s_ref, d_ref, pay_ref = refs
    far = jnp.where(backward, count - 1 - here, here)
    dec = [unpacked(p[STATE_ROWS:, :]) for p in pieces]

    def chosen(values, k):
        return jnp.where(backward, values[(count - k) % count], values[k])

    steps = [chosen(dec, k) for k in range(count)]
    mine_d = jnp.ones((8, LANES), F32)
    for k in range(1, count):
        mine_d = mine_d * jnp.where(far >= k, steps[k], 1.0)
    total_d = steps[0]
    for k in range(1, count):
        total_d = total_d * steps[k]
    for t in range(TILES):
        rows = slice(t * 64, t * 64 + 64)
        states = [p[rows, :].astype(F32) for p in pieces]
        ordered = [chosen(states, k) for k in range(count)]
        row = slice(t, t + 1)
        mine = jnp.zeros((64, LANES), F32)
        for k in range(count - 1, 0, -1):
            mine = jnp.where(far >= k, mine * steps[k][row] + ordered[k], mine)
        if last:
            in_ref[rows, :] = (mine * carry_d[row, :] + carry_s[rows, :]).astype(BF16)
            continue
        run = mine * steps[0][row] + ordered[0]
        for k in range(count - 1, 0, -1):
            run = jnp.where(far < k, run * steps[k][row] + ordered[k], run)
        s_ref[rows, :] = mine
        pay_ref[rows, :] = run.astype(BF16)
    if not last:
        d_ref[...] = mine_d
        pay_ref[STATE_ROWS:, :] = packed([total_d[:TILES]])


def from_each(x, axis, tiles=None):
    count = lax.axis_size(axis)
    return [
        lax.ppermute(x if tiles is None else tiles[j], axis, [(i, (i + j) % count) for i in range(count)])
        for j in range(1, count)
    ]


VMEM = pl.BlockSpec(memory_space=pltpu.VMEM)
HBM = pl.BlockSpec(memory_space=pltpu.HBM)


def in_hbm(x):
    return pltpu.with_memory_space_constraint(x, pltpu.HBM)


def small_call(kernel, name, shapes, *arrays, scratch=(), flops=0):
    return pl.pallas_call(
        kernel,
        out_shape=shapes,
        in_specs=[VMEM] * len(arrays),
        out_specs=jax.tree.map(lambda _: VMEM, shapes),
        scratch_shapes=scratch,
        cost_estimate=pl.CostEstimate(flops=flops, bytes_accessed=2**20, transcendentals=0),
        compiler_params=pltpu.CompilerParams(vmem_limit_bytes=8 * 2**20),
        name=name,
    )(*arrays)


def mix_kernel(n_out_ref, n_qr_ref, w_out_ref, w_qr_ref, in_ref, pieces_ref, gates_ref, *refs):
    *tile_refs, mixed_ref = refs
    low = lax.broadcasted_iota(jnp.int32, (1, LANES), 1) < 64
    low2 = (lax.broadcasted_iota(jnp.int32, (1, 2 * LANES), 1) % LANES) < 64

    core = lax.axis_index("sp_2")
    dec = [unpacked(pieces_ref[d, d, STATE_ROWS:, :]) for d in range(2)]

    def entering(tile):
        rows = slice(tile * 64, tile * 64 + 64)
        parts = []
        for d in range(2):
            chip = in_ref[d, rows, :].astype(F32)
            past = chip * dec[d][tile : tile + 1] + pieces_ref[d, d, rows, :].astype(F32)
            parts.append(jnp.where(core == d, chip, past))
        return jnp.concatenate(parts, axis=1)

    zero = jnp.zeros((64, 2 * LANES), F32)
    for u in range(4):
        if u < 2:
            s = entering(u)
            s = jnp.concatenate([jnp.where(low2, s, 0.0), jnp.where(low2, 0.0, s)], axis=0)
            o = dot_t(n_qr_ref[u], s.astype(BF16)) + n_out_ref[u]
        else:
            t = 2 + 2 * (u - 2)
            o = w_out_ref[u - 2] + dot_t(w_qr_ref[t - 2], jnp.concatenate([entering(t), zero], axis=0).astype(BF16))
            o = o + dot_t(w_qr_ref[t - 1], jnp.concatenate([zero, entering(t + 1)], axis=0).astype(BF16))
        square = o * o
        first = jnp.sum(jnp.where(low, square, 0.0), axis=-1, keepdims=True)
        second = jnp.sum(jnp.where(low, 0.0, square), axis=-1, keepdims=True)
        scale = lax.rsqrt(jnp.where(low, first, second) * (1.0 / 64) + EPS)
        mixed = o * scale * gates_ref[u]
        mixed_ref[:, u * LANES : (u + 1) * LANES] = mixed.astype(BF16)
    count, rows = len(tile_refs), tile_refs[0].shape[0]
    for j, tile_ref in enumerate(tile_refs):
        place = lax.rem(lax.axis_index("tp") + j, count)
        tile_ref[...] = mixed_ref[pl.ds(place * rows, rows), :]


def earlier_in_block(size, rows, axis):
    ri = lax.broadcasted_iota(jnp.int32, (size, size), 0)
    ci = lax.broadcasted_iota(jnp.int32, (size, size), 1)
    first, second = (ri, ci) if axis == 0 else (ci, ri)
    same = (ri // rows) == (ci // rows)
    return same, same & (first < second)


def slots_of(col, row, capacity, rows, axis):
    same, earlier = earlier_in_block(col[0].shape[0], rows, axis)
    own = row if axis == 0 else col
    other = col if axis == 0 else row

    def count(hit):
        return jnp.sum(jnp.where(hit, 1.0, 0.0), axis=axis, keepdims=True).astype(jnp.int32)

    rank0 = count((own[0] == other[0]) & earlier)
    rank1 = count((own[1] == other[1]) & earlier) + count((own[1] == other[0]) & same)
    return own[0] * capacity + rank0, own[1] * capacity + rank1


def picks_kernel(experts, capacity, copies, routes_ref, score_ref, after_ref, pick_ref, chosen_ref, table_ref):
    del after_ref
    rows = chosen_ref.shape[1]
    table = jnp.concatenate(
        [routes_ref[...].astype(F32), score_ref[...], jnp.zeros((4, routes_ref.shape[1]), F32)], axis=0
    )
    table_ref[...] = jnp.transpose(table)
    table = table_ref[pl.ds(lax.axis_index("tp") * rows, rows), :]
    table_t = jnp.transpose(table)
    col = [table[:, k : k + 1].astype(jnp.int32) for k in range(2)]
    row = [table_t[k : k + 1, :].astype(jnp.int32) for k in range(2)]
    slots = slots_of(col, row, capacity, rows, 1)
    s0, s1 = table[:, 2:3], table[:, 3:4]
    weights = (1.0 / (1.0 + jnp.exp(s1 - s0)), 1.0 / (1.0 + jnp.exp(s0 - s1)))
    j = lax.broadcasted_iota(jnp.int32, (rows, experts * copies * capacity), 1)
    code = (j // (copies * capacity)) * capacity + j % capacity
    hits = [code == slot for slot in slots]
    pick = jnp.where(hits[0], weights[0], 0.0) + jnp.where(hits[1], weights[1], 0.0)
    high = pick.astype(BF16)
    pick_ref[:rows, :] = high
    pick_ref[rows:, :] = (pick - high.astype(F32)).astype(BF16)
    j = lax.broadcasted_iota(jnp.int32, (rows, experts * capacity), 1)
    chosen = jnp.where((j == slots[0]) | (j == slots[1]), 1.0, 0.0)
    chosen_ref[...] = jnp.transpose(chosen).astype(BF16)


def route_kernel(
    x0_ref, x1_ref, x2_ref, x3_ref, w_ref, stream_ref, gain_ref, chosen_ref, res_ref, buf_ref
):
    rows, width = res_ref.shape
    experts, copies, capacity, _ = buf_ref.shape
    here = lax.axis_index("tp")
    residual = stream_ref[pl.ds(here * rows, rows), :].astype(F32)
    span = 2 * LANES
    for j, x_ref in enumerate((x0_ref, x1_ref, x2_ref, x3_ref)):
        source = lax.rem(here + copies - j, copies)
        for g in range(2):
            part = x_ref[:, g * span : (g + 1) * span]
            residual = residual + dot(part, w_ref[g, pl.ds(source * span, span), :])
    res_ref[...] = residual
    mean = jnp.mean(residual * residual, axis=-1, keepdims=True)
    norm = (residual * lax.rsqrt(mean + EPS) * gain_ref[...]).astype(BF16)
    sent = dot(chosen_ref[...], norm).astype(BF16).reshape(experts, capacity, width)
    for t in range(copies):
        buf_ref[:, t] = sent


def final_kernel(pick_ref, back_ref, res_ref, o_ref):
    rows = res_ref.shape[0]
    both = dot(pick_ref[...], back_ref[...])
    o_ref[...] = (res_ref[...] + both[:rows] + both[rows:]).astype(BF16)


def local(
    stream,
    narrow_query_weight,
    wide_query_weight,
    value_rows_heads,
    output_gate_logits,
    narrow_forget_logits,
    wide_forget_logits,
    narrow_forget_headroom,
    wide_forget_headroom,
    extra_log_decay,
    per_head_norm_gain,
    mixer_output_weight,
    feedforward_norm_gain,
    expert_gate_matrix,
    expert_up_matrix,
    expert_down_matrix,
    routes,
    router_scores_chosen,
):
    nf, wf = in_hbm(narrow_forget_logits), in_hbm(wide_forget_logits)
    nh, wh = in_hbm(narrow_forget_headroom), in_hbm(wide_forget_headroom)
    nq, wq = in_hbm(narrow_query_weight), in_hbm(wide_query_weight)
    extra, values = in_hbm(extra_log_decay.transpose(1, 2, 0)), in_hbm(value_rows_heads)

    def from_hbm(kernel, name, inputs, shapes, vmem, after=(), kept=0, flops=0):
        buffered = inputs[: len(inputs) - kept]
        return pl.pallas_call(
            kernel,
            out_shape=shapes,
            in_specs=[HBM] * len(inputs) + [VMEM] * len(after),
            out_specs=jax.tree.map(lambda _: VMEM, shapes),
            scratch_shapes=[pltpu.VMEM(x.shape, x.dtype) for x in buffered]
            + [pltpu.SemaphoreType.DMA((len(inputs),))],
            compiler_params=pltpu.CompilerParams(vmem_limit_bytes=vmem * 2**20),
            cost_estimate=pl.CostEstimate(
                flops=flops, bytes_accessed=3 * 2**20, transcendentals=2 * 10**6
            ),
            name=name,
        )(*inputs, *after)

    payload = from_hbm(
        states_kernel, "local_states", (nf, nh, extra, values, wf, wh),
        jax.ShapeDtypeStruct((2, PAY_ROWS, LANES), BF16), 12, flops=10**9,
    )
    states = jax.ShapeDtypeStruct((STATE_ROWS, LANES), F32)
    decays = jax.ShapeDtypeStruct((8, LANES), F32)
    half = jax.ShapeDtypeStruct((PAY_ROWS, LANES), BF16)
    own = jax.ShapeDtypeStruct((2, TOK, LANES), F32)

    def queries(count):
        return jax.ShapeDtypeStruct((count, TOK, 2 * LANES), BF16)

    pieces = lax.all_gather(payload, "sp_2")
    chip = small_call(pair_kernel, "pair", half, pieces)
    chips = [chip, *from_each(chip, "sp_1")]
    wide, wide_q, token = from_hbm(
        wide_kernel, "wide_outputs", (wf, wh, extra, values, wq), (own, queries(4), decays), 20,
        after=(chip,), flops=3 * 10**9,
    )
    s, d, row = small_call(
        partial(level_kernel, lax.axis_size("sp_1"), "sp_1", False), "level_1", (states, decays, half),
        token, *chips,
    )
    rows_ = [row, *from_each(row, "sp_0")]
    narrow, narrow_q, gates, mixer_weight = from_hbm(
        narrow_kernel, "narrow_outputs",
        (nf, nh, extra, values, nq, in_hbm(output_gate_logits), in_hbm(mixer_output_weight)),
        (
            own, queries(2), jax.ShapeDtypeStruct((4, TOK, LANES), F32),
            pltpu.VMEM(mixer_output_weight.shape, BF16),
        ),
        20, after=(per_head_norm_gain.reshape(1, 64), d), kept=1,
        flops=3 * 10**9,
    )
    entering = small_call(
        partial(level_kernel, lax.axis_size("sp_0"), "sp_0", True), "level_0",
        jax.ShapeDtypeStruct((STATE_ROWS, LANES), BF16), *rows_, s, d,
    )
    entering = lax.all_gather(entering, "sp_2")
    tp = lax.axis_size("tp")
    rows = TOK // tp
    tiles = small_call(
        mix_kernel, "mix", (jax.ShapeDtypeStruct((rows, 4 * LANES), BF16),) * tp, narrow, narrow_q,
        wide, wide_q, entering, pieces, gates,
        scratch=[pltpu.VMEM((TOK, 4 * LANES), BF16)],
    )
    width = stream.shape[1]
    experts = lax.axis_size(SP)
    capacity = max(2, 2 * routes.shape[1] * rows // experts)
    slots = experts * tp * capacity
    pick, chosen = small_call(
        partial(picks_kernel, experts, capacity, tp), "picks",
        (
            jax.ShapeDtypeStruct((2 * rows, slots), BF16),
            jax.ShapeDtypeStruct((experts * capacity, rows), BF16),
        ),
        routes.T, router_scores_chosen.T, d, scratch=[pltpu.VMEM((TOK, 8), F32)],
        flops=10**9,
    )
    arrived = [tiles[0]] + from_each(None, "tp", tiles)
    residual, buffers = pl.pallas_call(
        route_kernel,
        out_shape=(
            jax.ShapeDtypeStruct((rows, width), F32),
            jax.ShapeDtypeStruct((experts, tp, capacity, width), BF16),
        ),
        in_specs=[VMEM] * 8,
        out_specs=(VMEM,) * 2,
        compiler_params=pltpu.CompilerParams(vmem_limit_bytes=20 * 2**20),
        name="project_and_route",
    )(
        *arrived, mixer_weight, stream, feedforward_norm_gain.reshape(1, width), chosen,
    )
    buffers = buffers.reshape(slots, width)
    tokens = lax.all_to_all(buffers, SP_TP, 0, 0, tiled=True)
    gate = jnp.dot(tokens, expert_gate_matrix[0], preferred_element_type=F32)
    up = jnp.dot(tokens, expert_up_matrix[0], preferred_element_type=F32)
    hidden = (jax.nn.silu(gate) * up).astype(BF16)
    part = jnp.dot(hidden, expert_down_matrix[0], preferred_element_type=F32).astype(BF16)
    back = lax.all_to_all(part, SP_TP, 0, 0, tiled=True)
    return pl.pallas_call(
        final_kernel,
        in_specs=[VMEM] * 3,
        out_specs=VMEM,
        out_shape=jax.ShapeDtypeStruct((rows, width), BF16),
        compiler_params=pltpu.CompilerParams(vmem_limit_bytes=12 * 2**20),
        name="combine",
    )(pick, back, residual)


def solution(mesh):
    torus = Mesh(mesh.devices.reshape(4, 4, 2, mesh.shape["tp"]), ("sp_0", "sp_1", "sp_2", "tp"))
    return jax.shard_map(
        local,
        mesh=torus,
        in_specs=(
            P(SP, None),
            P(SP, "tp"),
            P(SP, "tp"),
            P(SP, None, "tp"),
            P(SP, None, "tp"),
            P(None, SP, "tp"),
            P(None, SP, "tp"),
            P(None, "tp"),
            P(None, "tp"),
            P(SP, None, "tp"),
            P(),
            P(),
            P(),
            P(SP, None, "tp"),
            P(SP, None, "tp"),
            P(SP, "tp", None),
            P(SP, None),
            P(SP, None),
        ),
        out_specs=P(SP_TP, None),
        check_vma=False,
    )
```

```python
from functools import partial

import jax
import jax.numpy as jnp
from jax import lax
from jax.experimental import pallas as pl
from jax.experimental.pallas import tpu as pltpu
from jax.sharding import Mesh
from jax.sharding import PartitionSpec as P

SP = ("sp_0", "sp_1", "sp_2")
SP_TP = ("sp_0", "sp_1", "sp_2", "tp")

EPS = 1e-06
F32 = jnp.float32
BF16 = jnp.bfloat16

TOK = 256
BLK = 64
NB = TOK // BLK
LANES = 128
TILES = 6
STATE_ROWS = TILES * 64
PAY_ROWS = STATE_ROWS + 16


def dot(a, b):
    return lax.dot_general(a, b, (((1,), (0,)), ((), ())), preferred_element_type=F32)


def dot_t(a, b):
    return lax.dot_general(a, b, (((1,), (1,)), ((), ())), preferred_element_type=F32)


def silu(x):
    return x / (1.0 + jnp.exp(-x))


def copied(sources, targets, sems):
    copies = [
        pltpu.make_async_copy(a, b, sems.at[i]) for i, (a, b) in enumerate(zip(sources, targets))
    ]
    for copy in copies:
        copy.start()
    return copies


class Tiles:
    def __init__(self, ex_ref):
        ri = lax.broadcasted_iota(jnp.int32, (TOK, TOK), 0)
        ci = lax.broadcasted_iota(jnp.int32, (TOK, TOK), 1)
        self.same = (ri // BLK) == (ci // BLK)
        self.tri = (self.same & (ci <= ri), self.same & (ci >= ri))
        self.ones = tuple(jnp.where(t, 1.0, 0.0).astype(BF16) for t in self.tri)
        self.low = lax.broadcasted_iota(jnp.int32, (1, LANES), 1) < 64
        self.low2 = (lax.broadcasted_iota(jnp.int32, (1, 2 * LANES), 1) % LANES) < 64
        self.ex = jnp.transpose(jnp.concatenate([ex_ref[0], ex_ref[1]], axis=0))

    def extra(self, tile):
        if tile >= 2:
            return self.ex[:, tile + 2 : tile + 3]
        return jnp.where(
            self.low, self.ex[:, 2 * tile : 2 * tile + 1], self.ex[:, 2 * tile + 1 : 2 * tile + 2]
        )

    def decayed(self, tile, d, f_raw, room):
        opening = room / (1.0 + jnp.exp(f_raw.astype(F32)))
        ld = jnp.log(1.0 - opening) + self.extra(tile)
        hi = ld.astype(BF16)
        lo = (ld - hi.astype(F32)).astype(BF16)
        both = dot(self.ones[d], jnp.concatenate([hi, lo], axis=1))
        inside = (both[:, :LANES] + both[:, LANES:]).reshape(NB, BLK, LANES)
        edge = BLK - 1 if d == 0 else 0
        end = [inside[b, edge : edge + 1, :] for b in range(NB)]
        start = [None] * NB
        run = jnp.zeros((1, LANES), F32)
        for b in range(NB) if d == 0 else reversed(range(NB)):
            start[b] = run
            run = run + end[b]
        opening = opening.reshape(NB, BLK, LANES)
        ke = (opening * jnp.exp(jnp.stack(end, axis=0) - inside)).reshape(TOK, LANES).astype(BF16)
        return opening, inside, [jnp.exp(e) for e in end], jnp.stack(start, axis=0), run, ke

    def block_values(self, tile, v, ke):
        vt = jnp.transpose(v.astype(F32))

        def spread(part):
            return jnp.where(self.same, jnp.concatenate([part] * NB, axis=0), 0.0).astype(BF16)

        if tile >= 2:
            half = (tile % 2) * 64
            return dot(spread(vt[half : half + 64]), ke)
        return jnp.where(self.low2, dot(spread(vt[:64]), ke), dot(spread(vt[64:]), ke))

    def swept(self, kv, ends):
        states = [[None, None] for _ in range(NB)]
        closing = []
        for d in range(2):
            run = jnp.zeros((64, LANES), F32)
            for b in range(NB) if d == 0 else reversed(range(NB)):
                states[b][d] = run
                run = run * ends[d][b] + kv[b * 64 : b * 64 + 64, d * LANES : (d + 1) * LANES]
            closing.append(run)
        return [jnp.concatenate(s, axis=1) for s in states], closing


def place_of(tile):
    if tile < 2:
        return slice(tile * LANES, (tile + 1) * LANES), slice(tile * LANES, (tile + 1) * LANES)
    h = tile - 2
    return slice(h * LANES, (h + 1) * LANES), slice(h // 2 * LANES, (h // 2 + 1) * LANES)


def states_kernel(
    nf_hbm, nh_hbm, ex_hbm, v_hbm, wf_hbm, wh_hbm, pay_ref, nf_ref, nh_ref, ex_ref, v_ref, wf_ref,
    wh_ref, sems,
):
    copies = copied(
        (nf_hbm, nh_hbm, ex_hbm, v_hbm, wf_hbm, wh_hbm),
        (nf_ref, nh_ref, ex_ref, v_ref, wf_ref, wh_ref),
        sems,
    )
    for copy in copies[:4]:
        copy.wait()
    tiles = Tiles(ex_ref)
    decays = [[], []]
    for tile in range(TILES):
        if tile == 2:
            for copy in copies[4:]:
                copy.wait()
        cols, v_cols = place_of(tile)
        f_ref, h_ref = (nf_ref, nh_ref) if tile < 2 else (wf_ref, wh_ref)
        ke, ends = [], []
        for d in range(2):
            _, _, end, _, total, k = tiles.decayed(tile, d, f_ref[d, :, cols], h_ref[d : d + 1, cols])
            ke.append(k)
            ends.append(end)
            decays[d].append(jnp.exp(total))
        kv = tiles.block_values(tile, v_ref[:, 0 if tile < 2 else 1, v_cols], jnp.concatenate(ke, axis=1))
        _, closing = tiles.swept(kv, ends)
        for d in range(2):
            pay_ref[d, tile * 64 : tile * 64 + 64, :] = closing[d].astype(BF16)
    for d in range(2):
        pay_ref[d, STATE_ROWS:, :] = packed(decays[d])


def narrow_kernel(
    nf_hbm, nh_hbm, ex_hbm, v_hbm, nq_hbm, gate_hbm, w_hbm, gain_ref, after_ref, out_ref, qr_ref,
    gates_ref, w_ref, nf_ref, nh_ref, ex_ref, v_ref, nq_ref, gate_ref, sems,
):
    del after_ref
    copies = copied(
        (nf_hbm, nh_hbm, ex_hbm, v_hbm, nq_hbm, gate_hbm, w_hbm),
        (nf_ref, nh_ref, ex_ref, v_ref, nq_ref, gate_ref, w_ref), sems,
    )
    for copy in copies[:-1]:
        copy.wait()
    own_outputs(0, nf_ref, nh_ref, ex_ref, v_ref, nq_ref, out_ref, qr_ref)
    gain = jnp.concatenate([gain_ref[...], gain_ref[...]], axis=1)
    for u in range(4):
        c = (u % 2) * LANES
        gates_ref[u] = silu(gate_ref[:, u // 2, c : c + LANES].astype(F32)) * gain
    copies[-1].wait()


def wide_kernel(
    wf_hbm, wh_hbm, ex_hbm, v_hbm, wq_hbm, after_ref, out_ref, qr_ref, token_ref,
    wf_ref, wh_ref, ex_ref, v_ref, wq_ref, sems,
):
    del after_ref
    for copy in copied(
        (wf_hbm, wh_hbm, ex_hbm, v_hbm, wq_hbm), (wf_ref, wh_ref, ex_ref, v_ref, wq_ref), sems
    ):
        copy.wait()
    own_outputs(1, wf_ref, wh_ref, ex_ref, v_ref, wq_ref, out_ref, qr_ref)
    token_ref[...] = jnp.zeros(token_ref.shape, F32)


def own_outputs(group, f_ref, h_ref, ex_ref, v_ref, q_ref, out_ref, qr_ref):
    tiles = Tiles(ex_ref)
    low, low2 = tiles.low, tiles.low2

    def prepare(tile):
        cols, v_cols = place_of(tile)
        q = silu(q_ref[:, cols].astype(F32)).reshape(NB, BLK, LANES)
        qi, ki, ke, qr, ends = [], [], [], [], []
        for d in range(2):
            opening, inside, end, start, _, k = tiles.decayed(
                tile, d, f_ref[d, :, cols], h_ref[d : d + 1, cols]
            )
            qi.append((q * jnp.exp(inside)).reshape(TOK, LANES))
            qr.append((q * jnp.exp(inside + start)).reshape(TOK, LANES).astype(BF16))
            ki.append((opening * jnp.exp(-inside)).reshape(TOK, LANES))
            ke.append(k)
            ends.append(end)
        qr_ref[tile - 2 * group] = jnp.concatenate(qr, axis=1)
        v = v_ref[:, group, v_cols]
        states, _ = tiles.swept(tiles.block_values(tile, v, jnp.concatenate(ke, axis=1)), ends)
        return qi, ki, states, v

    def scores(qi, ki):
        total = jnp.where(tiles.tri[0], dot_t(qi[0].astype(BF16), ki[0].astype(BF16)), 0.0)
        total = total + jnp.where(tiles.tri[1], dot_t(qi[1].astype(BF16), ki[1].astype(BF16)), 0.0)
        return total.astype(BF16)

    def joined(qi):
        return jnp.concatenate([x.astype(BF16) for x in qi], axis=1)

    for p in range(2) if group == 0 else ():
        qi, ki, states, v = prepare(p)
        q_cat = joined(qi)
        parts = []
        for b in range(NB):
            s = jnp.concatenate(
                [jnp.where(low2, states[b], 0.0), jnp.where(low2, 0.0, states[b])], axis=0
            )
            parts.append(dot_t(q_cat[b * BLK : (b + 1) * BLK], s.astype(BF16)))
        first = dot(scores(qi, [jnp.where(low, k, 0.0) for k in ki]), v)
        second = dot(scores(qi, [jnp.where(low, 0.0, k) for k in ki]), v)
        out_ref[p] = jnp.where(low, first, second) + jnp.concatenate(parts, axis=0)

    for p in range(2) if group == 1 else ():
        inner, q_cats, head_states = [], [], []
        for tile in (2 + 2 * p, 3 + 2 * p):
            qi, ki, states, v = prepare(tile)
            head_states.append(states)
            q_cats.append(joined(qi))
            inner.append(dot(scores(qi, ki), v))
        parts = []
        for b in range(NB):
            s = jnp.concatenate([head_states[0][b], head_states[1][b]], axis=0).astype(BF16)
            rows = slice(b * BLK, (b + 1) * BLK)
            parts.append(
                jnp.where(low, dot_t(q_cats[0][rows], s), dot_t(q_cats[1][rows], s))
            )
        out_ref[p] = jnp.where(low, inner[0], inner[1]) + jnp.concatenate(parts, axis=0)


def packed(rows):
    dec = jnp.concatenate(rows + [jnp.zeros((8 - TILES, LANES), F32)], axis=0)
    high = dec.astype(BF16).astype(F32)
    return jnp.concatenate([high, dec - high], axis=0).astype(BF16)


def unpacked(rows):
    rows = rows.astype(F32)
    return rows[:8] + rows[8:]


def pair_kernel(pieces_ref, pay_ref):
    core = lax.axis_index("sp_2")
    first, second = pieces_ref[core, core], pieces_ref[1 - core, core]
    d0, d1 = unpacked(first[STATE_ROWS:]), unpacked(second[STATE_ROWS:])
    for t in range(TILES):
        rows = slice(t * 64, t * 64 + 64)
        total = first[rows].astype(F32) * d1[t : t + 1] + second[rows].astype(F32)
        pay_ref[rows, :] = total.astype(BF16)
    both = d0 * d1
    pay_ref[STATE_ROWS:, :] = packed([both[:TILES]])


def level_kernel(count, axis, last, *refs):
    if not last:
        refs = refs[1:]
    pieces, refs = refs[:count], refs[count:]
    backward = lax.axis_index("sp_2") == 1
    here = lax.axis_index(axis)
    if last:
        carry_s, carry_d, in_ref = refs
    else:
        s_ref, d_ref, pay_ref = refs
    far = jnp.where(backward, count - 1 - here, here)
    dec = [unpacked(p[STATE_ROWS:, :]) for p in pieces]

    def chosen(values, k):
        return jnp.where(backward, values[(count - k) % count], values[k])

    steps = [chosen(dec, k) for k in range(count)]
    mine_d = jnp.ones((8, LANES), F32)
    for k in range(1, count):
        mine_d = mine_d * jnp.where(far >= k, steps[k], 1.0)
    total_d = steps[0]
    for k in range(1, count):
        total_d = total_d * steps[k]
    for t in range(TILES):
        rows = slice(t * 64, t * 64 + 64)
        states = [p[rows, :].astype(F32) for p in pieces]
        ordered = [chosen(states, k) for k in range(count)]
        row = slice(t, t + 1)
        mine = jnp.zeros((64, LANES), F32)
        for k in range(count - 1, 0, -1):
            mine = jnp.where(far >= k, mine * steps[k][row] + ordered[k], mine)
        if last:
            in_ref[rows, :] = (mine * carry_d[row, :] + carry_s[rows, :]).astype(BF16)
            continue
        run = mine * steps[0][row] + ordered[0]
        for k in range(count - 1, 0, -1):
            run = jnp.where(far < k, run * steps[k][row] + ordered[k], run)
        s_ref[rows, :] = mine
        pay_ref[rows, :] = run.astype(BF16)
    if not last:
        d_ref[...] = mine_d
        pay_ref[STATE_ROWS:, :] = packed([total_d[:TILES]])


def from_each(x, axis, tiles=None):
    count = lax.axis_size(axis)
    return [
        lax.ppermute(x if tiles is None else tiles[j], axis, [(i, (i + j) % count) for i in range(count)])
        for j in range(1, count)
    ]


VMEM = pl.BlockSpec(memory_space=pltpu.VMEM)
HBM = pl.BlockSpec(memory_space=pltpu.HBM)


def in_hbm(x):
    return pltpu.with_memory_space_constraint(x, pltpu.HBM)


def small_call(kernel, name, shapes, *arrays, scratch=(), flops=0):
    return pl.pallas_call(
        kernel,
        out_shape=shapes,
        in_specs=[VMEM] * len(arrays),
        out_specs=jax.tree.map(lambda _: VMEM, shapes),
        scratch_shapes=scratch,
        cost_estimate=pl.CostEstimate(flops=flops, bytes_accessed=2**20, transcendentals=0),
        compiler_params=pltpu.CompilerParams(vmem_limit_bytes=8 * 2**20),
        name=name,
    )(*arrays)


def mix_kernel(n_out_ref, n_qr_ref, w_out_ref, w_qr_ref, in_ref, pieces_ref, gates_ref, *refs):
    *tile_refs, mixed_ref = refs
    low = lax.broadcasted_iota(jnp.int32, (1, LANES), 1) < 64
    low2 = (lax.broadcasted_iota(jnp.int32, (1, 2 * LANES), 1) % LANES) < 64

    core = lax.axis_index("sp_2")
    dec = [unpacked(pieces_ref[d, d, STATE_ROWS:, :]) for d in range(2)]

    def entering(tile):
        rows = slice(tile * 64, tile * 64 + 64)
        parts = []
        for d in range(2):
            chip = in_ref[d, rows, :].astype(F32)
            past = chip * dec[d][tile : tile + 1] + pieces_ref[d, d, rows, :].astype(F32)
            parts.append(jnp.where(core == d, chip, past))
        return jnp.concatenate(parts, axis=1)

    zero = jnp.zeros((64, 2 * LANES), F32)
    for u in range(4):
        if u < 2:
            s = entering(u)
            s = jnp.concatenate([jnp.where(low2, s, 0.0), jnp.where(low2, 0.0, s)], axis=0)
            o = dot_t(n_qr_ref[u], s.astype(BF16)) + n_out_ref[u]
        else:
            t = 2 + 2 * (u - 2)
            o = w_out_ref[u - 2] + dot_t(w_qr_ref[t - 2], jnp.concatenate([entering(t), zero], axis=0).astype(BF16))
            o = o + dot_t(w_qr_ref[t - 1], jnp.concatenate([zero, entering(t + 1)], axis=0).astype(BF16))
        square = o * o
        first = jnp.sum(jnp.where(low, square, 0.0), axis=-1, keepdims=True)
        second = jnp.sum(jnp.where(low, 0.0, square), axis=-1, keepdims=True)
        scale = lax.rsqrt(jnp.where(low, first, second) * (1.0 / 64) + EPS)
        mixed = o * scale * gates_ref[u]
        mixed_ref[:, u * LANES : (u + 1) * LANES] = mixed.astype(BF16)
    count, rows = len(tile_refs), tile_refs[0].shape[0]
    for j, tile_ref in enumerate(tile_refs):
        place = lax.rem(lax.axis_index("tp") + j, count)
        tile_ref[...] = mixed_ref[pl.ds(place * rows, rows), :]


def earlier_in_block(size, rows, axis):
    ri = lax.broadcasted_iota(jnp.int32, (size, size), 0)
    ci = lax.broadcasted_iota(jnp.int32, (size, size), 1)
    first, second = (ri, ci) if axis == 0 else (ci, ri)
    same = (ri // rows) == (ci // rows)
    return same, same & (first < second)


def slots_of(col, row, capacity, rows, axis):
    same, earlier = earlier_in_block(col[0].shape[0], rows, axis)
    own = row if axis == 0 else col
    other = col if axis == 0 else row

    def count(hit):
        return jnp.sum(jnp.where(hit, 1.0, 0.0), axis=axis, keepdims=True).astype(jnp.int32)

    rank0 = count((own[0] == other[0]) & earlier)
    rank1 = count((own[1] == other[1]) & earlier) + count((own[1] == other[0]) & same)
    return own[0] * capacity + rank0, own[1] * capacity + rank1


def picks_kernel(experts, capacity, copies, routes_ref, score_ref, after_ref, pick_ref, chosen_ref, table_ref):
    del after_ref
    rows = chosen_ref.shape[1]
    table = jnp.concatenate(
        [routes_ref[...].astype(F32), score_ref[...], jnp.zeros((4, routes_ref.shape[1]), F32)], axis=0
    )
    table_ref[...] = jnp.transpose(table)
    table = table_ref[pl.ds(lax.axis_index("tp") * rows, rows), :]
    table_t = jnp.transpose(table)
    col = [table[:, k : k + 1].astype(jnp.int32) for k in range(2)]
    row = [table_t[k : k + 1, :].astype(jnp.int32) for k in range(2)]
    slots = slots_of(col, row, capacity, rows, 1)
    s0, s1 = table[:, 2:3], table[:, 3:4]
    weights = (1.0 / (1.0 + jnp.exp(s1 - s0)), 1.0 / (1.0 + jnp.exp(s0 - s1)))
    j = lax.broadcasted_iota(jnp.int32, (rows, experts * copies * capacity), 1)
    code = (j // (copies * capacity)) * capacity + j % capacity
    hits = [code == slot for slot in slots]
    pick = jnp.where(hits[0], weights[0], 0.0) + jnp.where(hits[1], weights[1], 0.0)
    high = pick.astype(BF16)
    pick_ref[:rows, :] = high
    pick_ref[rows:, :] = (pick - high.astype(F32)).astype(BF16)
    j = lax.broadcasted_iota(jnp.int32, (rows, experts * capacity), 1)
    chosen = jnp.where((j == slots[0]) | (j == slots[1]), 1.0, 0.0)
    chosen_ref[...] = jnp.transpose(chosen).astype(BF16)


def route_kernel(
    x0_ref, x1_ref, x2_ref, x3_ref, w_ref, stream_ref, gain_ref, chosen_ref, res_ref, buf_ref
):
    rows, width = res_ref.shape
    experts, copies, capacity, _ = buf_ref.shape
    here = lax.axis_index("tp")
    residual = stream_ref[pl.ds(here * rows, rows), :].astype(F32)
    span = 2 * LANES
    for j, x_ref in enumerate((x0_ref, x1_ref, x2_ref, x3_ref)):
        source = lax.rem(here + copies - j, copies)
        for g in range(2):
            part = x_ref[:, g * span : (g + 1) * span]
            residual = residual + dot(part, w_ref[g, pl.ds(source * span, span), :])
    res_ref[...] = residual
    mean = jnp.mean(residual * residual, axis=-1, keepdims=True)
    norm = (residual * lax.rsqrt(mean + EPS) * gain_ref[...]).astype(BF16)
    sent = dot(chosen_ref[...], norm).astype(BF16).reshape(experts, capacity, width)
    for t in range(copies):
        buf_ref[:, t] = sent


def final_kernel(pick_ref, back_ref, res_ref, o_ref):
    rows = res_ref.shape[0]
    both = dot(pick_ref[...], back_ref[...])
    o_ref[...] = (res_ref[...] + both[:rows] + both[rows:]).astype(BF16)


def local(
    stream,
    narrow_query_weight,
    wide_query_weight,
    value_rows_heads,
    output_gate_logits,
    narrow_forget_logits,
    wide_forget_logits,
    narrow_forget_headroom,
    wide_forget_headroom,
    extra_log_decay,
    per_head_norm_gain,
    mixer_output_weight,
    feedforward_norm_gain,
    expert_gate_matrix,
    expert_up_matrix,
    expert_down_matrix,
    routes,
    router_scores_chosen,
):
    nf, wf = in_hbm(narrow_forget_logits), in_hbm(wide_forget_logits)
    nh, wh = in_hbm(narrow_forget_headroom), in_hbm(wide_forget_headroom)
    nq, wq = in_hbm(narrow_query_weight), in_hbm(wide_query_weight)
    extra, values = in_hbm(extra_log_decay.transpose(1, 2, 0)), in_hbm(value_rows_heads)

    def from_hbm(kernel, name, inputs, shapes, vmem, after=(), kept=0, flops=0):
        buffered = inputs[: len(inputs) - kept]
        return pl.pallas_call(
            kernel,
            out_shape=shapes,
            in_specs=[HBM] * len(inputs) + [VMEM] * len(after),
            out_specs=jax.tree.map(lambda _: VMEM, shapes),
            scratch_shapes=[pltpu.VMEM(x.shape, x.dtype) for x in buffered]
            + [pltpu.SemaphoreType.DMA((len(inputs),))],
            compiler_params=pltpu.CompilerParams(vmem_limit_bytes=vmem * 2**20),
            cost_estimate=pl.CostEstimate(
                flops=flops, bytes_accessed=3 * 2**20, transcendentals=2 * 10**6
            ),
            name=name,
        )(*inputs, *after)

    payload = from_hbm(
        states_kernel, "local_states", (nf, nh, extra, values, wf, wh),
        jax.ShapeDtypeStruct((2, PAY_ROWS, LANES), BF16), 12, flops=10**9,
    )
    states = jax.ShapeDtypeStruct((STATE_ROWS, LANES), F32)
    decays = jax.ShapeDtypeStruct((8, LANES), F32)
    half = jax.ShapeDtypeStruct((PAY_ROWS, LANES), BF16)
    own = jax.ShapeDtypeStruct((2, TOK, LANES), F32)

    def queries(count):
        return jax.ShapeDtypeStruct((count, TOK, 2 * LANES), BF16)

    pieces = lax.all_gather(payload, "sp_2")
    chip = small_call(pair_kernel, "pair", half, pieces)
    chips = [chip, *from_each(chip, "sp_1")]
    wide, wide_q, token = from_hbm(
        wide_kernel, "wide_outputs", (wf, wh, extra, values, wq), (own, queries(4), decays), 20,
        after=(chip,), flops=3 * 10**9,
    )
    s, d, row = small_call(
        partial(level_kernel, lax.axis_size("sp_1"), "sp_1", False), "level_1", (states, decays, half),
        token, *chips,
    )
    rows_ = [row, *from_each(row, "sp_0")]
    narrow, narrow_q, gates, mixer_weight = from_hbm(
        narrow_kernel, "narrow_outputs",
        (nf, nh, extra, values, nq, in_hbm(output_gate_logits), in_hbm(mixer_output_weight)),
        (
            own, queries(2), jax.ShapeDtypeStruct((4, TOK, LANES), F32),
            pltpu.VMEM(mixer_output_weight.shape, BF16),
        ),
        20, after=(per_head_norm_gain.reshape(1, 64), d), kept=1,
        flops=3 * 10**9,
    )
    entering = small_call(
        partial(level_kernel, lax.axis_size("sp_0"), "sp_0", True), "level_0",
        jax.ShapeDtypeStruct((STATE_ROWS, LANES), BF16), *rows_, s, d,
    )
    entering = lax.all_gather(entering, "sp_2")
    tp = lax.axis_size("tp")
    rows = TOK // tp
    tiles = small_call(
        mix_kernel, "mix", (jax.ShapeDtypeStruct((rows, 4 * LANES), BF16),) * tp, narrow, narrow_q,
        wide, wide_q, entering, pieces, gates,
        scratch=[pltpu.VMEM((TOK, 4 * LANES), BF16)],
    )
    width = stream.shape[1]
    experts = lax.axis_size(SP)
    capacity = max(2, 2 * routes.shape[1] * rows // experts)
    slots = experts * tp * capacity
    pick, chosen = small_call(
        partial(picks_kernel, experts, capacity, tp), "picks",
        (
            jax.ShapeDtypeStruct((2 * rows, slots), BF16),
            jax.ShapeDtypeStruct((experts * capacity, rows), BF16),
        ),
        routes.T, router_scores_chosen.T, d, scratch=[pltpu.VMEM((TOK, 8), F32)],
        flops=10**9,
    )
    arrived = [tiles[0]] + from_each(None, "tp", tiles)
    residual, buffers = pl.pallas_call(
        route_kernel,
        out_shape=(
            jax.ShapeDtypeStruct((rows, width), F32),
            jax.ShapeDtypeStruct((experts, tp, capacity, width), BF16),
        ),
        in_specs=[VMEM] * 8,
        out_specs=(VMEM,) * 2,
        compiler_params=pltpu.CompilerParams(vmem_limit_bytes=20 * 2**20),
        name="project_and_route",
    )(
        *arrived, mixer_weight, stream, feedforward_norm_gain.reshape(1, width), chosen,
    )
    buffers = buffers.reshape(slots, width)
    tokens = lax.all_to_all(buffers, SP_TP, 0, 0, tiled=True)
    gate = jnp.dot(tokens, expert_gate_matrix[0], preferred_element_type=F32)
    up = jnp.dot(tokens, expert_up_matrix[0], preferred_element_type=F32)
    hidden = (jax.nn.silu(gate) * up).astype(BF16)
    part = jnp.dot(hidden, expert_down_matrix[0], preferred_element_type=F32).astype(BF16)
    back = lax.all_to_all(part, SP_TP, 0, 0, tiled=True)
    return pl.pallas_call(
        final_kernel,
        in_specs=[VMEM] * 3,
        out_specs=VMEM,
        out_shape=jax.ShapeDtypeStruct((rows, width), BF16),
        compiler_params=pltpu.CompilerParams(vmem_limit_bytes=12 * 2**20),
        name="combine",
    )(pick, back, residual)


def solution(mesh):
    torus = Mesh(mesh.devices.reshape(4, 4, 2, mesh.shape["tp"]), ("sp_0", "sp_1", "sp_2", "tp"))
    return jax.shard_map(
        local,
        mesh=torus,
        in_specs=(
            P(SP, None),
            P(SP, "tp"),
            P(SP, "tp"),
            P(SP, None, "tp"),
            P(SP, None, "tp"),
            P(None, SP, "tp"),
            P(None, SP, "tp"),
            P(None, "tp"),
            P(None, "tp"),
            P(SP, None, "tp"),
            P(),
            P(),
            P(),
            P(SP, None, "tp"),
            P(SP, None, "tp"),
            P(SP, "tp", None),
            P(SP, None),
            P(SP, None),
        ),
        out_specs=P(SP_TP, None),
        check_vma=False,
    )
```
